512 devices in a mesh: kv: 64 (over z, y), tp: 8 (over x, core).
Axes of the slice: x: 4, y: 4, z: 16, core: 2. Of those that a mesh axis runs over, the one named last changes fastest.
Arguments:
- stream: bfloat16 [32, 4096], P(None, 'kv'), may hold values from -32 to 32
- gain_in: bfloat16 [4096], P('kv'), may hold values from 0.099609375 to 1.8984375
- w_query: bfloat16 [4096, 2048], P('kv', 'tp'), may hold values from -0.09375 to 0.09375
- w_key: bfloat16 [4096, 2048], P('kv', 'tp'), may hold values from -0.09375 to 0.09375
- w_value: bfloat16 [4096, 2048], P('kv', 'tp'), may hold values from -0.09375 to 0.09375
- w_forget: bfloat16 [4096, 16], replicated, may hold values from -0.09375 to 0.09375
- keys_cache: bfloat16 [32, 16, 8192, 128], P(None, 'tp', 'kv'), may hold values from -136 to 136
- values_cache: bfloat16 [32, 16, 8192, 128], P(None, 'tp', 'kv'), may hold values from -6 to 6
- decay_cache: float32 [32, 16, 8192], P(None, 'tp', 'kv'), may hold values from -1283 to 0
- lengths: int32 [32], replicated, may hold values from 1 to 8192, 104889 in all
- gain_att: bfloat16 [2048], P('tp'), may hold values from 0.099609375 to 1.8984375
- w_out: bfloat16 [2048, 4096], P('tp', 'kv'), may hold values from -0.125 to 0.125
- gain_mlp: bfloat16 [4096], P('kv'), may hold values from 0.099609375 to 1.8984375
- w_up: bfloat16 [4096, 16384], P('kv', 'tp'), may hold values from -0.09375 to 0.09375
- w_down: bfloat16 [16384, 4096], P('tp', 'kv'), may hold values from -0.046875 to 0.046875
Outputs:
- updated: bfloat16 [32, 4096], P(None, 'kv')
The draws below stay inside these ranges and needn't reach their ends.
Inputs may be any that keep to these rules, and one draw needn't show every extreme that they name: `lengths`: one sequence has all 8192 positions live.
All inputs are finite; a program needn't handle non-finite values.
Results may differ from the reference program's by a relative error of at most 0.012.
The reference program's roundings to bfloat16 on the way count: a program that leaves them out, or rounds other values in their place, can miss the bound.
Values may be sent and summed in bfloat16 or wider, within the bound.
A program may use at most 64 MiB of HBM per device.

```python
import math
import jax
import jax.numpy as jnp
import numpy as np
from jax import lax

D = 4096
HEAD_COUNT = 16
HEAD_WIDTH = 128
FF = 16384
SEQUENCE_COUNT = 32
POS_DEV = 128
CACHE_LENGTH = 8192
HW = 2048


def draw_stream(key, part):
    key_one, key_two = jax.random.split(jax.random.fold_in(key, 11), 2)
    column = jnp.arange(D, dtype=jnp.float32) / D
    raw_values = jnp.clip(jax.random.normal(key_one, (SEQUENCE_COUNT, D), jnp.float32), -5.0, 5.0)
    column_scale = jnp.exp(math.log(10.0) * (column - 0.5))
    row_scale = jnp.exp(jax.random.uniform(key_two, (SEQUENCE_COUNT, 1), jnp.float32, math.log(0.5), math.log(2.0)))
    return (raw_values * column_scale[None, :] * row_scale).astype(jnp.bfloat16)


def draw_keys_cache(key, part):
    key_one = jax.random.fold_in(jax.random.fold_in(key, 5), 0)
    full_shape = (SEQUENCE_COUNT, HEAD_COUNT, CACHE_LENGTH, HEAD_WIDTH)
    raw_values = jnp.clip(jax.random.normal(key_one, full_shape, jnp.float32), -5.0, 5.0)
    return raw_values.astype(jnp.bfloat16)


def draw_decay_cache(key, part):
    every_key = jax.random.split(jax.random.fold_in(key, 23), 7)
    head_order = jax.random.permutation(every_key[0], HEAD_COUNT)
    keep_count = HEAD_COUNT // 2
    slow_heads = (head_order < keep_count).reshape(1, HEAD_COUNT, 1)
    slow_rate = jax.random.uniform(every_key[1], (SEQUENCE_COUNT, HEAD_COUNT, 1), jnp.float32, 0.2, 0.8) / CACHE_LENGTH
    fast_rate = 1.0 / (POS_DEV * jax.random.uniform(every_key[2], (SEQUENCE_COUNT, HEAD_COUNT, 1), jnp.float32, 0.25, 0.8))
    learning_rate = jnp.where(slow_heads, slow_rate, fast_rate)
    jaggedness = jnp.exp(jax.random.uniform(every_key[3], (SEQUENCE_COUNT, HEAD_COUNT, CACHE_LENGTH), jnp.float32, math.log(0.5), math.log(2.0)))
    block_count = CACHE_LENGTH // POS_DEV
    block_multiplier = jnp.exp(jax.random.uniform(every_key[4], (1, HEAD_COUNT, block_count, 1), jnp.float32, math.log(0.4), math.log(2.5)))
    block_multiplier = jnp.broadcast_to(block_multiplier, (1, HEAD_COUNT, block_count, POS_DEV)).reshape(1, HEAD_COUNT, CACHE_LENGTH)
    spike_position = jax.random.randint(every_key[5], (SEQUENCE_COUNT, HEAD_COUNT, 3, 1), 0, CACHE_LENGTH)
    spike_penalty = jnp.log(jax.random.uniform(every_key[6], (SEQUENCE_COUNT, HEAD_COUNT, 3, 1), jnp.float32, 0.5, 0.8))
    cache_positions = jnp.arange(CACHE_LENGTH, dtype=jnp.int32)
    spike_events = jnp.sum(jnp.where(cache_positions[None, None, None, :] == spike_position, spike_penalty, 0.0), axis=2)
    gate_logarithms = spike_events - learning_rate * jaggedness * block_multiplier
    suffix_sum = jnp.flip(jnp.cumsum(jnp.flip(gate_logarithms, 2), axis=2), 2)
    return suffix_sum - gate_logarithms


def shard_levels(own_key, extent, cuts, least, high):
    factor_of = 1.0
    for dim, shards_of in cuts:
        steps = jax.random.uniform(jax.random.fold_in(jax.random.fold_in(own_key, 6), dim), (shards_of,), jnp.float32, least / len(cuts), high / len(cuts))
        factor_of = factor_of * jnp.repeat(jnp.exp(steps), extent[dim] // shards_of).reshape((-1,) + (1,) * (len(extent) - 1 - dim))
    return factor_of


def profile(amount, total, bound, skew):
    portions = [(1 << 20) // math.isqrt(grade ** skew) + 1 for grade in range(2, amount + 1)]
    rest, given = total - bound - (amount - 1), [1] * (amount - 1)
    while rest > 0:
        movable = [i for i in range(amount - 1) if given[i] < bound]
        whole, budget = sum([portions[i] for i in movable]), rest
        for i in movable:
            extra = min(bound - given[i], max(1, budget * portions[i] // whole), rest)
            given[i] = given[i] + extra
            rest = rest - extra
    return np.array([bound] + given)


def ragged(stream_key, count, total, reach, slope):
    if count == 2:
        one = jax.random.randint(stream_key, (), max(1, total - reach), min(reach, total - 1) + 1)
        return jnp.stack([one, total - one])
    tallies = jnp.asarray(profile(count, total, reach, slope), jnp.int32)
    couples = (count - 1) // 2
    source_of, receiver = tallies[1:1 + 2 * couples:2], tallies[2:2 + 2 * couples:2]
    slack = jnp.minimum(source_of - 1, reach - receiver)
    moved = jax.random.randint(jax.random.fold_in(stream_key, 1), (couples,), 0, 1 << 20) % (slack + 1)
    tallies = tallies.at[1:1 + 2 * couples:2].set(source_of - moved).at[2:2 + 2 * couples:2].set(receiver + moved)
    return tallies[jax.random.permutation(jax.random.fold_in(stream_key, 2), count)]


def noise(key, dims, spread, bound, shards=(), kind=jnp.bfloat16):
    entries = spread * jax.random.normal(key, dims, jnp.float32)
    if shards:
        entries = entries * shard_levels(key, dims, shards, -0.22, 0.18)
    return jnp.clip(entries, -bound, bound).astype(kind)


def setup_inputs(seed: int = 0) -> dict:
    splits = jax.random.split(jax.random.key(seed), 16)
    stream = draw_stream(jax.random.fold_in(splits[15], 71), 0)
    gain_in = jnp.clip(1.0 + 0.18 * jax.random.normal(splits[1], (D,), jnp.float32), 0.099609375, 1.8984375).astype(jnp.bfloat16)
    w_query = noise(splits[2], (D, HW), D ** -0.5, 0.09375, ((0, 64), (1, 8)))
    w_key = noise(splits[3], (D, HW), D ** -0.5, 0.09375, ((0, 64), (1, 8)))
    w_value = noise(splits[4], (D, HW), D ** -0.5, 0.09375, ((0, 64), (1, 8)))
    w_forget = noise(splits[5], (D, HEAD_COUNT), D ** -0.5, 0.09375)
    keys_cache = draw_keys_cache(jax.random.fold_in(splits[15], 71), 0)
    values_cache = noise(splits[7], (SEQUENCE_COUNT, HEAD_COUNT, CACHE_LENGTH, HEAD_WIDTH), 1.0, 6.0, ((1, 8), (2, 64)))
    decay_cache = draw_decay_cache(jax.random.fold_in(splits[15], 71), 0)
    lengths = ragged(splits[9], SEQUENCE_COUNT, SEQUENCE_COUNT * CACHE_LENGTH * 2 // 5 + SEQUENCE_COUNT, CACHE_LENGTH, 2).astype(jnp.int32)
    gain_att = jnp.clip(1.0 + 0.18 * jax.random.normal(splits[10], (HW,), jnp.float32), 0.099609375, 1.8984375).astype(jnp.bfloat16)
    w_out = noise(splits[11], (HW, D), HW ** -0.5, 0.125, ((0, 8), (1, 64)))
    gain_mlp = jnp.clip(1.0 + 0.18 * jax.random.normal(splits[12], (D,), jnp.float32), 0.099609375, 1.8984375).astype(jnp.bfloat16)
    w_up = noise(splits[13], (D, FF), D ** -0.5, 0.09375, ((0, 64), (1, 8)))
    w_down = noise(splits[14], (FF, D), FF ** -0.5, 0.046875, ((0, 8), (1, 64)))
    return {"stream": stream, "gain_in": gain_in, "w_query": w_query, "w_key": w_key, "w_value": w_value, "w_forget": w_forget, "keys_cache": keys_cache, "values_cache": values_cache, "decay_cache": decay_cache, "lengths": lengths, "gain_att": gain_att, "w_out": w_out, "gain_mlp": gain_mlp, "w_up": w_up, "w_down": w_down}


norm_eps = 1e-06
masked_score = -1e+30

def head_blocks(head_index, queries, forget, keys_cache, values_cache, decay_cache, lengths):
    block_count = CACHE_LENGTH // POS_DEV
    head_queries = lax.dynamic_index_in_dim(queries, head_index, 1, False).astype(jnp.float32)
    head_keys = lax.dynamic_index_in_dim(keys_cache, head_index, 1, False).astype(jnp.float32)
    value_head = lax.dynamic_index_in_dim(values_cache, head_index, 1, False).astype(jnp.float32)
    decay_head = lax.dynamic_index_in_dim(decay_cache, head_index, 1, False)
    forget_head = lax.dynamic_index_in_dim(forget, head_index, 1, False)
    attention_logits = jnp.einsum('tk,txk->tx', head_queries, head_keys) * (1.0 / math.sqrt(HEAD_WIDTH))
    attention_logits = attention_logits + forget_head[:, None] + decay_head
    attention_logits = attention_logits.reshape(SEQUENCE_COUNT, block_count, POS_DEV)
    cache_positions = jnp.arange(CACHE_LENGTH, dtype=jnp.int32).reshape(block_count, POS_DEV)
    live_mask = cache_positions[None] < lengths.astype(jnp.int32)[:, None, None]
    attention_logits = jnp.where(live_mask, attention_logits, masked_score)
    block_peak = lax.optimization_barrier(jnp.max(attention_logits, axis=2))
    weights = jnp.where(live_mask, jnp.exp(attention_logits - block_peak[..., None]), 0.0)
    block_total = lax.optimization_barrier(jnp.sum(weights, axis=2))
    rounded = lax.optimization_barrier(weights.astype(jnp.bfloat16)).astype(jnp.float32)
    block_out = jnp.einsum('sbp,sbpd->sbd', rounded, value_head.reshape(SEQUENCE_COUNT, block_count, POS_DEV, HEAD_WIDTH))
    return (block_peak, block_total, block_out)

def reference(stream, gain_in, w_query, w_key, w_value, w_forget, keys_cache, values_cache, decay_cache, lengths, gain_att, w_out, gain_mlp, w_up, w_down):
    score_scale = 1.0 / math.sqrt(HEAD_WIDTH)
    stream_float = stream.astype(jnp.float32)
    scaled = (stream_float * gain_in.astype(jnp.float32)).astype(jnp.bfloat16)
    scale_in = lax.rsqrt(lax.optimization_barrier(jnp.mean(stream_float * stream_float, axis=1)) + norm_eps)[:, None]
    queries = (jnp.dot(scaled, w_query, preferred_element_type=jnp.float32) * scale_in).astype(jnp.bfloat16).reshape(SEQUENCE_COUNT, HEAD_COUNT, HEAD_WIDTH)
    key_new = (jnp.dot(scaled, w_key, preferred_element_type=jnp.float32) * scale_in).astype(jnp.bfloat16).reshape(SEQUENCE_COUNT, HEAD_COUNT, HEAD_WIDTH)
    value_new = (jnp.dot(scaled, w_value, preferred_element_type=jnp.float32) * scale_in).astype(jnp.bfloat16).reshape(SEQUENCE_COUNT, HEAD_COUNT, HEAD_WIDTH)
    forget = jax.nn.log_sigmoid(jnp.dot(scaled, w_forget, preferred_element_type=jnp.float32) * scale_in)
    block_peaks, totals, block_outs = lax.map(lambda head_index: head_blocks(head_index, queries, forget, keys_cache, values_cache, decay_cache, lengths), jnp.arange(HEAD_COUNT, dtype=jnp.int32))
    block_peaks = jnp.transpose(block_peaks, (1, 0, 2))
    totals = jnp.transpose(totals, (1, 0, 2))
    block_outs = jnp.transpose(block_outs, (1, 0, 2, 3))
    own_score = lax.optimization_barrier(jnp.sum(queries.astype(jnp.float32) * key_new.astype(jnp.float32), axis=2)) * score_scale
    top_score = jnp.maximum(lax.optimization_barrier(jnp.max(block_peaks, axis=2)), own_score)
    block_weight = jnp.exp(block_peaks - top_score[..., None])
    own_weight = jnp.exp(own_score - top_score)
    numerator = lax.optimization_barrier(jnp.sum(block_weight[..., None] * block_outs, axis=2)) + own_weight[..., None] * value_new.astype(jnp.float32)
    denominator = lax.optimization_barrier(jnp.sum(block_weight * totals, axis=2)) + own_weight
    attended = (numerator / denominator[..., None]).reshape(SEQUENCE_COUNT, HW)
    scale_att = lax.rsqrt(lax.optimization_barrier(jnp.mean(attended * attended, axis=1)) + norm_eps)[:, None]
    attended_in = (attended * gain_att.astype(jnp.float32)).astype(jnp.bfloat16)
    residual = (stream_float + scale_att * jnp.dot(attended_in, w_out, preferred_element_type=jnp.float32)).astype(jnp.bfloat16)
    residual_float = residual.astype(jnp.float32)
    mixer_in = (residual_float * gain_mlp.astype(jnp.float32)).astype(jnp.bfloat16)
    scale_mixer = lax.rsqrt(lax.optimization_barrier(jnp.mean(residual_float * residual_float, axis=1)) + norm_eps)[:, None]
    hidden = jnp.square(jax.nn.relu(jnp.dot(mixer_in, w_up, preferred_element_type=jnp.float32) * scale_mixer)).astype(jnp.bfloat16)
    return (residual_float + jnp.dot(hidden, w_down, preferred_element_type=jnp.float32)).astype(jnp.bfloat16)
```

```python
import math

import jax
import jax.numpy as jnp
from jax import lax
from jax.experimental import pallas as pl
from jax.experimental.pallas import tpu as pltpu
from jax.sharding import PartitionSpec as P

f32, bf16 = jnp.float32, jnp.bfloat16
MESH = pl.DeviceIdType.MESH
NORM_EPS = 1e-06
MASKED = -1e30

NZ, NY, NTP = 16, 4, 8
NKV = NZ * NY
SEQS, HEADS, HD, POS = 32, 2, 128, 128
COLS, UNITS = 64, 2048
D, HW = NKV * COLS, NTP * HEADS * HD
BLOCKS = UNITS // 128

QKV, QUERY, PART, ATT, OUT, UP, SQUARES, HIDDEN, DOWN = range(9)
EXCHANGES = 9


def kernel(
    stream_ref, gain_in_ref, wq_hbm, wk_hbm, wv_hbm, wf_hbm, keys_hbm, values_hbm, decay_ref,
    lengths_ref, gain_att_ref, wo_hbm, gain_mlp_ref, wu_hbm, wd_hbm,
    out_ref,
    wq, wk, wv, wf, keys, values, wo, wu, wd,
    len_buf, score_buf, prob_buf,
    send1, recv1, send_q, recv_q, send2, recv2, send_a, recv_a, send_o, recv_o,
    send_u, recv_u, send_s, recv_s, send_h, recv_h, send_d, recv_d,
    load_sem, send_sem, recv_sem,
):
    kv, tp = lax.axis_index("kv"), lax.axis_index("tp")
    z, y = kv // NY, lax.rem(kv, NY)

    def kv_peer(i):
        ring = i // NY
        dz = NZ // 2 + (1 - 2 * lax.rem(ring, 2)) * ((ring + 1) // 2)
        dy = i + i // (NKV - NY)
        return lax.rem(z + dz, NZ) * NY + lax.rem(y + dy, NY)

    def tp_peer(i):
        return lax.rem(tp + 1 + i, NTP)

    barrier = pltpu.get_barrier_semaphore()

    def greet_kv(i, c):
        pl.semaphore_signal(barrier, 1, device_id=(kv_peer(i), tp), device_id_type=MESH)
        return c

    def greet_tp(i, c):
        pl.semaphore_signal(barrier, 1, device_id=(kv, tp_peer(i)), device_id_type=MESH)
        return c

    lax.fori_loop(0, NKV - 1, greet_kv, 0)
    lax.fori_loop(0, NTP - 1, greet_tp, 0)

    rows = pl.ds(pl.multiple_of(kv * COLS, COLS), COLS)
    loads = [
        (wq_hbm, wq), (wk_hbm, wk), (wv_hbm, wv), (wf_hbm.at[rows, :], wf),
        (keys_hbm, keys), (values_hbm, values), (wo_hbm, wo), (wu_hbm, wu), (wd_hbm, wd),
    ]
    loads = [pltpu.make_async_copy(a, b, load_sem.at[k]) for k, (a, b) in enumerate(loads)]
    for load in loads:
        load.start()

    lane = lax.broadcasted_iota(jnp.int32, (SEQS, 128), 1)
    low_half = lane < 64

    def to_kv(name, source, target):
        def step(i, c):
            peer = kv_peer(i)
            pltpu.make_async_remote_copy(
                src_ref=source(peer), dst_ref=target, send_sem=send_sem.at[name],
                recv_sem=recv_sem.at[name], device_id=(peer, tp), device_id_type=MESH,
            ).start()
            return c

        lax.fori_loop(0, NKV - 1, step, 0)

    def to_tp(name, source, target):
        def step(i, c):
            pltpu.make_async_remote_copy(
                src_ref=source, dst_ref=target, send_sem=send_sem.at[name],
                recv_sem=recv_sem.at[name], device_id=(kv, tp_peer(i)), device_id_type=MESH,
            ).start()
            return c

        lax.fori_loop(0, NTP - 1, step, 0)

    def arrived(name, buffer):
        n = buffer.shape[0] - 1
        whole = buffer.at[pl.ds(0, n)]
        pltpu.make_async_copy(whole, whole, recv_sem.at[name]).wait()

    def sent(name, buffer):
        n = buffer.shape[0] - 1
        whole = buffer.at[pl.ds(0, n)]
        pltpu.make_async_copy(whole, whole, send_sem.at[name]).wait()

    stream = stream_ref[...].astype(f32)
    scaled = (stream * gain_in_ref[...].astype(f32)).astype(bf16)
    squares = jnp.sum(stream * stream, axis=1, keepdims=True)
    for s in range(SEQS):
        len_buf[s : s + 1, :] = jnp.full((1, 128), lengths_ref[s], jnp.int32)
    for k in range(4):
        loads[k].wait()
    part_f = jnp.dot(scaled, wf[...], preferred_element_type=f32)
    lane_f = lax.broadcasted_iota(jnp.int32, part_f.shape, 1)
    for r, w in enumerate((wq, wk, wv)):
        part = jnp.dot(scaled, w[...], preferred_element_type=f32)
        for h in range(HEADS):
            send1[h * SEQS : (h + 1) * SEQS, r, :] = part[:, h * HD : (h + 1) * HD]
    for h in range(HEADS):
        gate = jnp.sum(jnp.where(lane_f == tp * HEADS + h, part_f, 0.0), axis=1, keepdims=True)
        send1[h * SEQS : (h + 1) * SEQS, 3, :] = jnp.where(low_half, gate, squares)
    recv1[kv] = send1[kv]
    pl.semaphore_wait(barrier, NKV - 1 + NTP - 1)
    to_kv(QKV, lambda peer: send1.at[peer], recv1.at[kv])
    arrived(QKV, recv1)
    total = jnp.sum(recv1[...], axis=0)
    extra = total[3:4, :]
    lane_1 = lax.broadcasted_iota(jnp.int32, (1, 128), 1)
    gate_sum = jnp.sum(jnp.where(lane_1 == 0, extra, 0.0), axis=1, keepdims=True)
    square_sum = jnp.sum(jnp.where(lane_1 == 127, extra, 0.0), axis=1, keepdims=True)
    scale_in = lax.rsqrt(square_sum / D + NORM_EPS)
    query = (total[0:1, :] * scale_in).astype(bf16).astype(f32)
    send_q[...] = query
    recv_q[kv] = query
    to_kv(QUERY, lambda peer: send_q, recv_q.at[kv])
    key_new = (total[1:2, :] * scale_in).astype(bf16).astype(f32)
    value_new = (total[2:3, :] * scale_in).astype(bf16).astype(f32)
    gate_in = gate_sum * scale_in
    forget = jnp.minimum(gate_in, 0.0) - jnp.log1p(jnp.exp(-jnp.abs(gate_in)))
    score_scale = 1.0 / math.sqrt(HD)
    own = jnp.sum(query * key_new, axis=1, keepdims=True) * score_scale

    loads[4].wait()
    arrived(QUERY, recv_q)

    def score_rows(k, c):
        for h in range(HEADS):
            rows = []
            for j in range(8):
                q = recv_q[h * SEQS + k * 8 + j].astype(bf16)
                rows.append(
                    lax.dot_general(
                        q, keys[k * 8 + j, h], (((1,), (1,)), ((), ())), preferred_element_type=f32
                    )
                )
            at = pl.multiple_of(h * SEQS + k * 8, 8)
            score_buf[pl.ds(at, 8), :] = jnp.concatenate(rows, axis=0)
        return c

    lax.fori_loop(0, SEQS // 8, score_rows, 0)
    live = kv * POS + lane < len_buf[...]
    for h in range(HEADS):
        rows = slice(h * SEQS, (h + 1) * SEQS)
        logits = score_buf[rows, :] * score_scale + decay_ref[:, h, :]
        logits = jnp.where(live, logits, MASKED)
        peak = jnp.max(logits, axis=1, keepdims=True)
        probs = jnp.where(live, jnp.exp(logits - peak), 0.0)
        block_total = jnp.sum(probs, axis=1, keepdims=True)
        prob_buf[rows, :] = probs
        send2[rows, 1, :] = jnp.where(low_half, peak, block_total)
    loads[5].wait()

    def value_rows(k, c):
        for h in range(HEADS):
            at = pl.multiple_of(h * SEQS + k * 8, 8)
            probs = prob_buf[pl.ds(at, 8), :]
            for j in range(8):
                row = jnp.dot(
                    probs[j : j + 1, :].astype(bf16), values[k * 8 + j, h],
                    preferred_element_type=f32,
                )
                send2[h * SEQS + k * 8 + j, 0:1, :] = row
        return c

    lax.fori_loop(0, SEQS // 8, value_rows, 0)
    recv2[kv] = send2[kv]
    to_kv(PART, lambda peer: send2.at[peer], recv2.at[kv])
    arrived(PART, recv2)

    block_out, stats = recv2[:, 0, :], recv2[:, 1, :]
    low = lax.broadcasted_iota(jnp.int32, (NKV, 128), 1) < 64
    peaks = jnp.max(jnp.where(low, stats, 2 * MASKED), axis=1, keepdims=True) + forget
    totals = jnp.max(jnp.where(low, 0.0, stats), axis=1, keepdims=True)
    top = jnp.maximum(own, jnp.max(peaks, axis=0, keepdims=True))
    weight = jnp.exp(peaks - top)
    own_weight = jnp.exp(own - top)
    numerator = jnp.sum(weight * block_out, axis=0, keepdims=True) + own_weight * value_new
    denominator = jnp.sum(weight * totals, axis=0, keepdims=True) + own_weight
    attended = numerator / denominator
    send_a[...] = attended
    recv_a[kv] = attended
    to_kv(ATT, lambda peer: send_a, recv_a.at[kv])
    loads[6].wait()
    arrived(ATT, recv_a)

    part_out, att_squares = None, None
    for h in range(HEADS):
        att = recv_a[h * SEQS : (h + 1) * SEQS, 0, :]
        att_in = (att * gain_att_ref[h : h + 1, :].astype(f32)).astype(bf16)
        term = jnp.dot(att_in, wo[h * HD : (h + 1) * HD, :], preferred_element_type=f32)
        square = jnp.sum(att * att, axis=1, keepdims=True)
        part_out = term if h == 0 else part_out + term
        att_squares = square if h == 0 else att_squares + square
    send_o[...] = jnp.concatenate(
        [part_out, jnp.broadcast_to(att_squares, (SEQS, 128 - COLS))], axis=1
    )
    recv_o[tp] = send_o[...]
    to_tp(OUT, send_o, recv_o.at[tp])
    loads[7].wait()
    arrived(OUT, recv_o)
    out_total = jnp.sum(recv_o[...], axis=0)
    scale_att = lax.rsqrt(out_total[:, COLS : COLS + 1] / HW + NORM_EPS)
    residual = (stream + scale_att * out_total[:, :COLS]).astype(bf16).astype(f32)

    mixer_in = (residual * gain_mlp_ref[...].astype(f32)).astype(bf16)
    mixer_squares = jnp.sum(residual * residual, axis=1, keepdims=True)
    row = lax.broadcasted_iota(jnp.int32, (SEQS, 128), 0)
    as_row = jnp.sum(jnp.where(row == lane, mixer_squares, 0.0), axis=0, keepdims=True)
    send_s[...] = as_row
    recv_s[kv] = as_row
    to_kv(SQUARES, lambda peer: send_s, recv_s.at[kv])
    for u in range(BLOCKS):
        part = jnp.dot(mixer_in, wu[:, u * 128 : (u + 1) * 128], preferred_element_type=f32)
        send_u[u * 4 : (u + 1) * 4] = part.astype(bf16).reshape(4, 8, 128)
    recv_u[kv] = send_u[kv]
    to_kv(UP, lambda peer: send_u.at[peer], recv_u.at[kv])
    arrived(SQUARES, recv_s)
    square_row = jnp.sum(recv_s[...], axis=0)
    first = lax.rem(kv, 4) * 8
    pick = lax.broadcasted_iota(jnp.int32, (8, 128), 1) == first + lax.broadcasted_iota(
        jnp.int32, (8, 128), 0
    )
    mixer_total = jnp.sum(jnp.where(pick, square_row, 0.0), axis=1, keepdims=True)
    scale_mixer = lax.rsqrt(mixer_total / D + NORM_EPS)
    arrived(UP, recv_u)
    units = jnp.sum(recv_u[...].astype(f32), axis=0)
    active = jnp.maximum(units * scale_mixer, 0.0)
    hidden = (active * active).astype(bf16)
    send_h[...] = hidden
    recv_h[kv] = hidden
    to_kv(HIDDEN, lambda peer: send_h, recv_h.at[kv])
    loads[8].wait()
    arrived(HIDDEN, recv_h)

    part_down = None
    for u in range(BLOCKS):
        term = jnp.dot(
            recv_h[u * 4 : (u + 1) * 4].reshape(SEQS, 128), wd[u * 128 : (u + 1) * 128, :],
            preferred_element_type=f32,
        )
        part_down = term if u == 0 else part_down + term
    half = SEQS // 2
    send_d[...] = jnp.concatenate([part_down[:half], part_down[half:]], axis=1)
    recv_d[tp] = send_d[...]
    to_tp(DOWN, send_d, recv_d.at[tp])
    arrived(DOWN, recv_d)
    down = jnp.sum(recv_d[...], axis=0)
    down = jnp.concatenate([down[:, :COLS], down[:, COLS:]], axis=0)
    out_ref[...] = (residual + down).astype(bf16)

    for name, buffer in (
        (QKV, recv1), (QUERY, recv_q), (PART, recv2), (ATT, recv_a), (OUT, recv_o),
        (UP, recv_u), (SQUARES, recv_s), (HIDDEN, recv_h), (DOWN, recv_d),
    ):
        sent(name, buffer)


def per_device(
    stream, gain_in, w_query, w_key, w_value, w_forget, keys_cache, values_cache, decay_cache,
    lengths, gain_att, w_out, gain_mlp, w_up, w_down,
):
    vmem = pl.BlockSpec(memory_space=pltpu.VMEM)
    smem = pl.BlockSpec(memory_space=pltpu.SMEM)
    hbm = pl.BlockSpec(memory_space=pl.ANY)
    V = pltpu.VMEM
    scratch = [
        V((COLS, HEADS * HD), bf16), V((COLS, HEADS * HD), bf16), V((COLS, HEADS * HD), bf16),
        V((COLS, 16), bf16),
        V((SEQS, HEADS, POS, HD), bf16), V((SEQS, HEADS, POS, HD), bf16),
        V((HEADS * HD, COLS), bf16), V((COLS, UNITS), bf16), V((UNITS, COLS), bf16),
        V((SEQS, 128), jnp.int32), V((NKV, 128), f32), V((NKV, 128), f32),
        V((NKV, 4, 128), f32), V((NKV, 4, 128), f32),
        V((1, 128), f32), V((NKV, 1, 128), f32),
        V((NKV, 2, 128), f32), V((NKV, 2, 128), f32),
        V((1, 128), f32), V((NKV, 1, 128), f32),
        V((SEQS, 128), f32), V((NTP, SEQS, 128), f32),
        V((NKV, 8, 128), bf16), V((NKV, 8, 128), bf16),
        V((1, 128), f32), V((NKV, 1, 128), f32),
        V((8, 128), bf16), V((NKV, 8, 128), bf16),
        V((SEQS // 2, 128), f32), V((NTP, SEQS // 2, 128), f32),
        pltpu.SemaphoreType.DMA((9,)),
        pltpu.SemaphoreType.DMA((EXCHANGES,)), pltpu.SemaphoreType.DMA((EXCHANGES,)),
    ]
    return pl.pallas_call(
        kernel,
        out_shape=jax.ShapeDtypeStruct((SEQS, COLS), bf16),
        in_specs=[vmem, vmem, hbm, hbm, hbm, hbm, hbm, hbm, vmem, smem, vmem, hbm, vmem, hbm, hbm],
        out_specs=vmem,
        scratch_shapes=scratch,
        compiler_params=pltpu.CompilerParams(collective_id=0, has_side_effects=True),
    )(
        stream, gain_in.reshape(1, COLS), w_query, w_key, w_value, w_forget, keys_cache,
        values_cache, decay_cache, lengths, gain_att.reshape(HEADS, HD), w_out,
        gain_mlp.reshape(1, COLS), w_up, w_down,
    )


def solution(mesh):
    return jax.shard_map(
        per_device,
        mesh=mesh,
        in_specs=(
            P(None, "kv"), P("kv"), P("kv", "tp"), P("kv", "tp"), P("kv", "tp"), P(),
            P(None, "tp", "kv", None), P(None, "tp", "kv", None), P(None, "tp", "kv"), P(),
            P("tp"), P("tp", "kv"), P("kv"), P("kv", "tp"), P("tp", "kv"),
        ),
        out_specs=P(None, "kv"),
        check_vma=False,
    )
```

```python
import math

import jax
import jax.numpy as jnp
from jax import lax
from jax.experimental import pallas as pl
from jax.experimental.pallas import tpu as pltpu
from jax.sharding import PartitionSpec as P

f32, bf16 = jnp.float32, jnp.bfloat16
MESH = pl.DeviceIdType.MESH
NORM_EPS = 1e-06
MASKED = -1e30
NT = (((1,), (1,)), ((), ()))

NZ, NY, NTP = 16, 4, 8
NKV = NZ * NY
SEQS, HEADS, HD, POS = 32, 2, 128, 128
COLS, UNITS = 64, 2048
D, HW = NKV * COLS, NTP * HEADS * HD
BLOCKS = UNITS // 128

QKV, PART, ATT, OUT, OUT_SQ, UP, SQUARES, SCALE, HIDDEN, DOWN = range(10)
EXCHANGES = 10


def kernel(
    stream_hbm, gain_in_hbm, wq_hbm, wk_hbm, wv_hbm, wf_hbm, keys_hbm, values_hbm, decay_hbm,
    lengths_hbm, gain_att_hbm, wo_hbm, gain_mlp_hbm, wu_hbm, wd_hbm,
    out_ref,
    stream_ref, gain_in_ref, wq, wk, wv, wf, keys, values, decay_ref, lengths_ref, gain_att_ref,
    wo, gain_mlp_ref, wu, wd,
    len_buf, bias_buf,
    send1, recv1, send_q, recv_q, send2, recv2, send_a, recv_a, send_o, recv_o, send_os, recv_os,
    send_u, recv_u, send_s, recv_s, recv_t, send_h, recv_h, send_d, recv_d,
    load_sem, send_sem, recv_sem, query_send_sem, query_sem,
):
    kv, tp = lax.axis_index("kv"), lax.axis_index("tp")
    z, y = kv // NY, lax.rem(kv, NY)

    def away(i):
        ring = i // NY
        dz = NZ // 2 + (1 - 2 * lax.rem(ring, 2)) * ((ring + 1) // 2)
        return dz, i + i // (NKV - NY)

    def kv_peer(i):
        dz, dy = away(i)
        return lax.rem(z + dz, NZ) * NY + lax.rem(y + dy, NY)

    def tp_peer(i):
        return lax.rem(tp + 1 + i, NTP)

    barrier = pltpu.get_barrier_semaphore()

    def greet_kv(i, c):
        pl.semaphore_signal(barrier, 1, device_id=(kv_peer(i), tp), device_id_type=MESH)
        return c

    def greet_tp(i, c):
        pl.semaphore_signal(barrier, 1, device_id=(kv, tp_peer(i)), device_id_type=MESH)
        return c

    lax.fori_loop(0, NKV - 1, greet_kv, 0)
    lax.fori_loop(0, NTP - 1, greet_tp, 0)

    pair_cols = pl.ds(pl.multiple_of(kv // 2 * 128, 128), 128)
    loads = {
        "stream": (stream_hbm, stream_ref), "gain_in": (gain_in_hbm, gain_in_ref),
        "wf": (wf_hbm.at[:, pair_cols], wf), "wq": (wq_hbm, wq), "wk": (wk_hbm, wk),
        "wv": (wv_hbm, wv), "lengths": (lengths_hbm, lengths_ref),
        "decay": (decay_hbm, decay_ref), "keys": (keys_hbm, keys), "values": (values_hbm, values),
        "gain_att": (gain_att_hbm, gain_att_ref), "wo": (wo_hbm, wo),
        "gain_mlp": (gain_mlp_hbm, gain_mlp_ref), "wu": (wu_hbm, wu), "wd": (wd_hbm, wd),
    }
    loads = {
        name: pltpu.make_async_copy(a, b, load_sem.at[k])
        for k, (name, (a, b)) in enumerate(loads.items())
    }
    for load in loads.values():
        load.start()

    def loaded(*names):
        for name in names:
            loads[name].wait()

    lane = lax.broadcasted_iota(jnp.int32, (SEQS, 128), 1)
    low_half = lane < 64

    def to_kv(name, source, target):
        def step(i, c):
            peer = kv_peer(i)
            pltpu.make_async_remote_copy(
                src_ref=source(peer), dst_ref=target, send_sem=send_sem.at[name],
                recv_sem=recv_sem.at[name], device_id=(peer, tp), device_id_type=MESH,
            ).start()
            return c

        lax.fori_loop(0, NKV - 1, step, 0)

    def to_tp(name, source, target):
        def step(i, c):
            pltpu.make_async_remote_copy(
                src_ref=source, dst_ref=target, send_sem=send_sem.at[name],
                recv_sem=recv_sem.at[name], device_id=(kv, tp_peer(i)), device_id_type=MESH,
            ).start()
            return c

        lax.fori_loop(0, NTP - 1, step, 0)

    def arrived(name, buffer):
        n = buffer.shape[0] - 1
        whole = buffer.at[pl.ds(0, n)]
        pltpu.make_async_copy(whole, whole, recv_sem.at[name]).wait()

    def sent(name, buffer):
        n = buffer.shape[0] - 1
        whole = buffer.at[pl.ds(0, n)]
        pltpu.make_async_copy(whole, whole, send_sem.at[name]).wait()

    loaded("stream", "gain_in", "wf", "wq", "wk", "wv")
    stream = stream_ref[...].astype(f32)
    scaled = (stream * gain_in_ref[...].astype(f32)).astype(bf16)
    squares = jnp.sum(stream * stream, axis=1, keepdims=True)
    mine = low_half == (lax.rem(kv, 2) == 0)
    scaled_f = scaled.astype(f32)
    both = jnp.where(mine, jnp.concatenate([scaled_f, scaled_f], axis=1), 0.0).astype(bf16)
    part_f = lax.dot_general(both, wf[...], NT, preferred_element_type=f32)
    lane_f = lax.broadcasted_iota(jnp.int32, part_f.shape, 1)
    for r, w in enumerate((wq, wk, wv)):
        part = jnp.dot(scaled, w[...], preferred_element_type=f32)
        for h in range(HEADS):
            send1[h * SEQS : (h + 1) * SEQS, r, :] = part[:, h * HD : (h + 1) * HD]
    for h in range(HEADS):
        gate = jnp.sum(jnp.where(lane_f == tp * HEADS + h, part_f, 0.0), axis=1, keepdims=True)
        send1[h * SEQS : (h + 1) * SEQS, 3, :] = jnp.where(low_half, gate, squares)
    recv1[kv] = send1[kv]
    loaded("lengths", "decay")
    for s in range(SEQS):
        len_buf[s : s + 1, :] = jnp.full((1, 128), lengths_ref[s], jnp.int32)
    live = kv * POS + lane < len_buf[...]
    for h in range(HEADS):
        bias = jnp.where(live, decay_ref[:, h, :], MASKED)
        bias_buf[h * SEQS // NY : (h + 1) * SEQS // NY] = bias.reshape(SEQS // NY, NY, 128)
    loaded("keys", "values")
    pl.semaphore_wait(barrier, NKV - 1 + NTP - 1)
    to_kv(QKV, lambda peer: send1.at[peer], recv1.at[kv])
    arrived(QKV, recv1)
    total = jnp.sum(recv1[...], axis=0)
    extra = total[3:4, :]
    lane_1 = lax.broadcasted_iota(jnp.int32, (1, 128), 1)
    gate_sum = jnp.sum(jnp.where(lane_1 == 0, extra, 0.0), axis=1, keepdims=True)
    square_sum = jnp.sum(jnp.where(lane_1 == 127, extra, 0.0), axis=1, keepdims=True)
    scale_in = lax.rsqrt(square_sum / D + NORM_EPS)
    query = (total[0:1, :] * scale_in).astype(bf16).astype(f32)
    send_q[...] = query
    recv_q[kv] = query

    def send_query(i, c):
        dz, _ = away(i)
        pltpu.make_async_remote_copy(
            src_ref=send_q, dst_ref=recv_q.at[kv], send_sem=query_send_sem,
            recv_sem=query_sem.at[dz], device_id=(kv_peer(i), tp), device_id_type=MESH,
        ).start()
        return c

    lax.fori_loop(0, NKV - 1, send_query, 0)
    key_new = (total[1:2, :] * scale_in).astype(bf16).astype(f32)
    value_new = (total[2:3, :] * scale_in).astype(bf16).astype(f32)
    gate_in = gate_sum * scale_in
    forget = jnp.minimum(gate_in, 0.0) - jnp.log1p(jnp.exp(-jnp.abs(gate_in)))
    score_scale = 1.0 / math.sqrt(HD)
    own = jnp.sum(query * key_new, axis=1, keepdims=True) * score_scale

    def group(steps):
        zs = [lax.rem(z + NZ - dz, NZ) for dz in steps]
        pairs = []
        for dz, zs_ in zip(steps, zs):
            part = recv_q.at[pl.ds(0, NY if dz else NY - 1)]
            pltpu.make_async_copy(part, part, query_sem.at[dz]).wait()
            pairs += [(zs_ * NY + j, j, dz) for j in range(NY)]
        scores = []
        for p, _, _ in pairs:
            scores.append(
                lax.dot_general(
                    recv_q[p].astype(bf16), keys[lax.rem(p, SEQS), p // SEQS], NT,
                    preferred_element_type=f32,
                )
            )
        bias = jnp.concatenate([bias_buf[zs_] for zs_ in zs], axis=0)
        alive = bias > 0.5 * MASKED
        logits = jnp.concatenate(scores, axis=0) * score_scale + bias
        logits = jnp.where(alive, logits, MASKED)
        peak = jnp.max(logits, axis=1, keepdims=True)
        probs = jnp.where(alive, jnp.exp(logits - peak), 0.0)
        block_total = jnp.sum(probs, axis=1, keepdims=True)
        stats = jnp.where(low_half[: len(pairs)], peak, block_total)
        for k, (p, _, _) in enumerate(pairs):
            send2[p, 0:1, :] = jnp.dot(
                probs[k : k + 1].astype(bf16), values[lax.rem(p, SEQS), p // SEQS],
                preferred_element_type=f32,
            )
            send2[p, 1:2, :] = stats[k : k + 1]
        for p, j, dz in pairs:
            copy = pltpu.make_async_remote_copy(
                src_ref=send2.at[p], dst_ref=recv2.at[kv], send_sem=send_sem.at[PART],
                recv_sem=recv_sem.at[PART], device_id=(p, tp), device_id_type=MESH,
            )
            if dz:
                copy.start()
            else:
                pl.when(j != y)(copy.start)

    group([2, 14, 1, 15, 0])
    recv2[kv] = send2[kv]
    group([4, 12, 3, 13])
    group([6, 10, 5, 11])
    group([8, 7, 9])
    arrived(PART, recv2)
    block_out, stats = recv2[:, 0, :], recv2[:, 1, :]
    low = lax.broadcasted_iota(jnp.int32, (NKV, 128), 1) < 64
    peaks = jnp.max(jnp.where(low, stats, 2 * MASKED), axis=1, keepdims=True) + forget
    totals = jnp.max(jnp.where(low, 0.0, stats), axis=1, keepdims=True)
    top = jnp.maximum(own, jnp.max(peaks, axis=0, keepdims=True))
    weight = jnp.exp(peaks - top)
    own_weight = jnp.exp(own - top)
    numerator = jnp.sum(weight * block_out, axis=0, keepdims=True) + own_weight * value_new
    denominator = jnp.sum(weight * totals, axis=0, keepdims=True) + own_weight
    attended = numerator / denominator
    send_a[...] = attended
    recv_a[kv] = attended
    to_kv(ATT, lambda peer: send_a, recv_a.at[kv])
    loaded("wo", "gain_att", "gain_mlp", "wu", "wd")
    arrived(ATT, recv_a)

    part_out, att_squares = None, None
    for h in range(HEADS):
        att = recv_a[h * SEQS : (h + 1) * SEQS, 0, :]
        att_in = (att * gain_att_ref[h : h + 1, :].astype(f32)).astype(bf16)
        term = lax.dot_general(
            att_in, wo[:, h * HD : (h + 1) * HD], NT, preferred_element_type=f32
        )
        square = jnp.sum(att * att, axis=1, keepdims=True)
        part_out = term if h == 0 else part_out + term
        att_squares = square if h == 0 else att_squares + square
    row = lax.broadcasted_iota(jnp.int32, (SEQS, 128), 0)

    def as_row(column):
        return jnp.sum(jnp.where(row == lane, column, 0.0), axis=0, keepdims=True)

    def as_column(line):
        return jnp.sum(jnp.where(row == lane, line, 0.0), axis=1, keepdims=True)

    half = SEQS // 2
    send_o[...] = jnp.concatenate([part_out[:half], part_out[half:]], axis=1)
    send_os[...] = as_row(att_squares)
    recv_o[tp] = send_o[...]
    recv_os[tp] = send_os[...]
    to_tp(OUT, send_o, recv_o.at[tp])
    to_tp(OUT_SQ, send_os, recv_os.at[tp])
    arrived(OUT, recv_o)
    arrived(OUT_SQ, recv_os)
    out_total = jnp.sum(recv_o[...], axis=0)
    out_total = jnp.concatenate([out_total[:, :COLS], out_total[:, COLS:]], axis=0)
    scale_att = lax.rsqrt(as_column(jnp.sum(recv_os[...], axis=0)) / HW + NORM_EPS)
    residual = (stream + scale_att * out_total).astype(bf16).astype(f32)

    mixer_in = (residual * gain_mlp_ref[...].astype(f32)).astype(bf16)
    for u in range(BLOCKS):
        part = jnp.dot(mixer_in, wu[:, u * 128 : (u + 1) * 128], preferred_element_type=f32)
        send_u[u * 4 : (u + 1) * 4] = part.astype(bf16).reshape(4, 8, 128)
    recv_u[kv] = send_u[kv]
    to_kv(UP, lambda peer: send_u.at[peer], recv_u.at[kv])
    adder = lax.rem(kv, NTP) == tp
    send_s[...] = as_row(jnp.sum(residual * residual, axis=1, keepdims=True))

    def send_squares(j, c):
        peer = j * NTP + tp

        @pl.when(peer != kv)
        def _():
            pltpu.make_async_remote_copy(
                src_ref=send_s, dst_ref=recv_s.at[kv], send_sem=send_sem.at[SQUARES],
                recv_sem=recv_sem.at[SQUARES], device_id=(peer, tp), device_id_type=MESH,
            ).start()

        return c

    lax.fori_loop(0, NKV // NTP, send_squares, 0)
    arrived(UP, recv_u)
    active = jnp.maximum(jnp.sum(recv_u[...].astype(f32), axis=0), 0.0)
    hidden = (active * active).astype(bf16)
    send_h[...] = hidden
    recv_h[kv] = hidden
    to_kv(HIDDEN, lambda peer: send_h, recv_h.at[kv])

    @pl.when(adder)
    def _():
        arrived(SQUARES, recv_s)
        recv_s[kv] = send_s[...]
        recv_t[...] = jnp.sum(recv_s[...], axis=0)
        to_tp(SCALE, recv_t, recv_t)

    arrived(HIDDEN, recv_h)

    part_down = None
    for u in range(BLOCKS):
        term = lax.dot_general(
            recv_h[u * 4 : (u + 1) * 4].reshape(SEQS, 128), wd[:, u * 128 : (u + 1) * 128], NT,
            preferred_element_type=f32,
        )
        part_down = term if u == 0 else part_down + term
    send_d[...] = jnp.concatenate([part_down[:half], part_down[half:]], axis=1)
    recv_d[tp] = send_d[...]
    to_tp(DOWN, send_d, recv_d.at[tp])
    @pl.when(jnp.logical_not(adder))
    def _():
        pltpu.make_async_copy(recv_t, recv_t, recv_sem.at[SCALE]).wait()

    scale_mixer = lax.rsqrt(as_column(recv_t[...]) / D + NORM_EPS)
    arrived(DOWN, recv_d)
    down = jnp.sum(recv_d[...], axis=0)
    down = jnp.concatenate([down[:, :COLS], down[:, COLS:]], axis=0)
    out_ref[...] = (residual + scale_mixer * scale_mixer * down).astype(bf16)

    for name, buffer in (
        (QKV, recv1), (PART, recv2), (ATT, recv_a), (OUT, recv_o), (OUT_SQ, recv_os), (UP, recv_u),
        (HIDDEN, recv_h), (DOWN, recv_d),
    ):
        sent(name, buffer)
    queries = recv_q.at[pl.ds(0, NKV - 1)]
    pltpu.make_async_copy(queries, queries, query_send_sem).wait()
    rows_out = recv_s.at[pl.ds(0, NKV // NTP - 1)]
    pltpu.make_async_copy(rows_out, rows_out, send_sem.at[SQUARES]).wait()

    @pl.when(jnp.logical_not(adder))
    def _():
        pltpu.make_async_copy(send_s, send_s, send_sem.at[SQUARES]).wait()

    @pl.when(adder)
    def _():
        rows_out = recv_s.at[pl.ds(0, NTP - 1)]
        pltpu.make_async_copy(rows_out, rows_out, send_sem.at[SCALE]).wait()


def per_device(
    stream, gain_in, w_query, w_key, w_value, w_forget, keys_cache, values_cache, decay_cache,
    lengths, gain_att, w_out, gain_mlp, w_up, w_down,
):
    hbm = pl.BlockSpec(memory_space=pl.ANY)
    V = pltpu.VMEM
    scratch = [
        V((SEQS, COLS), bf16), V((1, COLS), bf16),
        V((COLS, HEADS * HD), bf16), V((COLS, HEADS * HD), bf16), V((COLS, HEADS * HD), bf16),
        V((16, 128), bf16),
        V((SEQS, HEADS, POS, HD), bf16), V((SEQS, HEADS, POS, HD), bf16),
        V((SEQS, HEADS, POS), f32), pltpu.SMEM((SEQS,), jnp.int32), V((HEADS, HD), bf16),
        V((COLS, HEADS * HD), bf16), V((1, COLS), bf16), V((COLS, UNITS), bf16),
        V((COLS, UNITS), bf16),
        V((SEQS, 128), jnp.int32), V((NZ, NY, 128), f32),
        V((NKV, 4, 128), f32), V((NKV, 4, 128), f32),
        V((1, 128), f32), V((NKV, 1, 128), f32),
        V((NKV, 2, 128), f32), V((NKV, 2, 128), f32),
        V((1, 128), f32), V((NKV, 1, 128), f32),
        V((SEQS // 2, 128), f32), V((NTP, SEQS // 2, 128), f32),
        V((1, 128), f32), V((NTP, 1, 128), f32),
        V((NKV, 8, 128), bf16), V((NKV, 8, 128), bf16),
        V((1, 128), f32), V((NKV, 1, 128), f32), V((1, 128), f32),
        V((8, 128), bf16), V((NKV, 8, 128), bf16),
        V((SEQS // 2, 128), f32), V((NTP, SEQS // 2, 128), f32),
        pltpu.SemaphoreType.DMA((15,)),
        pltpu.SemaphoreType.DMA((EXCHANGES,)), pltpu.SemaphoreType.DMA((EXCHANGES,)),
        pltpu.SemaphoreType.DMA, pltpu.SemaphoreType.DMA((NZ,)),
    ]
    return pl.pallas_call(
        kernel,
        out_shape=pltpu.VMEM((SEQS, COLS), bf16),
        in_specs=[hbm] * 15,
        out_specs=pl.BlockSpec(memory_space=pltpu.VMEM),
        scratch_shapes=scratch,
        compiler_params=pltpu.CompilerParams(collective_id=0, has_side_effects=True),
    )(
        stream, gain_in.reshape(1, COLS), w_query, w_key, w_value, w_forget.T, keys_cache,
        values_cache, decay_cache, lengths, gain_att.reshape(HEADS, HD), w_out.T,
        gain_mlp.reshape(1, COLS), w_up, w_down.T,
    )


def solution(mesh):
    return jax.shard_map(
        per_device,
        mesh=mesh,
        in_specs=(
            P(None, "kv"), P("kv"), P("kv", "tp"), P("kv", "tp"), P("kv", "tp"), P(),
            P(None, "tp", "kv", None), P(None, "tp", "kv", None), P(None, "tp", "kv"), P(),
            P("tp"), P("tp", "kv"), P("kv"), P("kv", "tp"), P("tp", "kv"),
        ),
        out_specs=P(None, "kv"),
        check_vma=False,
    )
```

```python
import math

import jax
import jax.numpy as jnp
from jax import lax
from jax.experimental import pallas as pl
from jax.experimental.pallas import tpu as pltpu
from jax.sharding import PartitionSpec as P

f32, bf16 = jnp.float32, jnp.bfloat16
MESH = pl.DeviceIdType.MESH
NORM_EPS = 1e-06
MASKED = -1e30
NT = (((1,), (1,)), ((), ()))

NZ, NY, NTP = 16, 4, 8
NKV = NZ * NY
GROUP = 16
FARS = NKV // GROUP
SEQS, HEADS, HD, POS = 32, 2, 128, 128
COLS, UNITS = 64, 2048
D, HW = NKV * COLS, NTP * HEADS * HD
BLOCKS = UNITS // 128

(
    QUERY_IN, REST_IN, SQ_IN, FAR_SQ_IN, QUERY, FAR_REST, PART, ATT, OUT, OUT_SQ,
    UP, SQ_MIX, FAR_UP, FAR_SQ_MIX, HIDDEN, DOWN,
) = range(16)
EXCHANGES = 16


def kernel(
    stream_hbm, gain_in_hbm, wq_hbm, wk_hbm, wv_hbm, wf_hbm, keys_hbm, values_hbm, decay_hbm,
    lengths_hbm, gain_att_hbm, wo_hbm, gain_mlp_hbm, wu_hbm, wd_hbm,
    out_ref,
    stream_ref, gain_in_ref, wq, wk, wv, wf, keys, values, decay_ref, lengths_ref, gain_att_ref,
    wo, gain_mlp_ref, wu, wd,
    len_buf, bias_buf, query_buf,
    send_qi, recv_qi, send_ri, recv_ri, send_si, recv_si, send_fsi, recv_fsi, send_q, recv_q, send_fr, recv_fr, rest_buf,
    send2, recv2, send_a, recv_a, send_o, recv_o, send_os, recv_os,
    send_u, recv_u, send_sm, recv_sm, send_fu, recv_fu, send_fsm, recv_fsm, send_h, recv_h,
    send_d, recv_d,
    load_sem, send_sem, recv_sem,
):
    kv, tp = lax.axis_index("kv"), lax.axis_index("tp")
    z, y = kv // NY, lax.rem(kv, NY)
    far, near = kv // GROUP, lax.rem(kv, GROUP)

    def kv_peer(i):
        ring = i // NY
        dz = NZ // 2 + (1 - 2 * lax.rem(ring, 2)) * ((ring + 1) // 2)
        dy = i + i // (NKV - NY)
        return lax.rem(z + dz, NZ) * NY + lax.rem(y + dy, NY)

    def tp_peer(i):
        return lax.rem(tp + 1 + i, NTP)

    barrier = pltpu.get_barrier_semaphore()

    def greet(kv_to, tp_to):
        pl.semaphore_signal(barrier, 1, device_id=(kv_to, tp_to), device_id_type=MESH)

    def greet_line(i, c):
        greet(lax.rem(z // 4 * 4 + 4 + lax.rem(i + 4, NZ - 4), NZ) * NY + y, tp)
        return c

    def greet_group(i, c):
        greet(far * GROUP + lax.rem(near + 1 + i, GROUP), tp)
        return c

    def greet_tp(i, c):
        greet(kv, tp_peer(i))
        return c

    lax.fori_loop(0, NZ - 4, greet_line, 0)
    lax.fori_loop(0, GROUP - 1, greet_group, 0)
    lax.fori_loop(0, NTP - 1, greet_tp, 0)

    pair_cols = pl.ds(pl.multiple_of(kv // 2 * 128, 128), 128)
    loads = {
        "stream": (stream_hbm, stream_ref), "gain_in": (gain_in_hbm, gain_in_ref),
        "wf": (wf_hbm.at[:, pair_cols], wf), "wq": (wq_hbm, wq), "wk": (wk_hbm, wk),
        "wv": (wv_hbm, wv), "lengths": (lengths_hbm, lengths_ref),
        "decay": (decay_hbm, decay_ref), "keys": (keys_hbm, keys), "values": (values_hbm, values),
        "gain_att": (gain_att_hbm, gain_att_ref), "wo": (wo_hbm, wo),
        "gain_mlp": (gain_mlp_hbm, gain_mlp_ref), "wu": (wu_hbm, wu), "wd": (wd_hbm, wd),
    }
    loads = {
        name: pltpu.make_async_copy(a, b, load_sem.at[k])
        for k, (name, (a, b)) in enumerate(loads.items())
    }
    for load in loads.values():
        load.start()

    def loaded(*names):
        for name in names:
            loads[name].wait()

    lane = lax.broadcasted_iota(jnp.int32, (SEQS, 128), 1)
    low_half = lane < 64

    def put(name, source, target, peer):
        pltpu.make_async_remote_copy(
            src_ref=source, dst_ref=target, send_sem=send_sem.at[name],
            recv_sem=recv_sem.at[name], device_id=(peer, tp), device_id_type=MESH,
        ).start()

    def to_kv(name, source, target):
        def step(i, c):
            put(name, source, target, kv_peer(i))
            return c

        lax.fori_loop(0, NKV - 1, step, 0)

    def to_group(name, source, target):
        def step(i, c):
            to = lax.rem(near + 1 + i, GROUP)
            put(name, source(to), target, far * GROUP + to)
            return c

        lax.fori_loop(0, GROUP - 1, step, 0)

    def to_far(name, source, target):
        for i in (2, 1, 3):
            to = lax.rem(far + i, FARS)
            put(name, source(to), target, to * GROUP + near)

    def to_tp(name, source, target):
        def step(i, c):
            pltpu.make_async_remote_copy(
                src_ref=source, dst_ref=target, send_sem=send_sem.at[name],
                recv_sem=recv_sem.at[name], device_id=(kv, tp_peer(i)), device_id_type=MESH,
            ).start()
            return c

        lax.fori_loop(0, NTP - 1, step, 0)

    def arrived(name, buffer):
        n = buffer.shape[0] - 1
        whole = buffer.at[pl.ds(0, n)]
        pltpu.make_async_copy(whole, whole, recv_sem.at[name]).wait()

    def sent(name, buffer):
        n = buffer.shape[0] - 1
        whole = buffer.at[pl.ds(0, n)]
        pltpu.make_async_copy(whole, whole, send_sem.at[name]).wait()

    row = lax.broadcasted_iota(jnp.int32, (SEQS, 128), 0)

    def as_row(column):
        return jnp.sum(jnp.where(row == lane, column, 0.0), axis=0, keepdims=True)

    def as_column(line):
        return jnp.sum(jnp.where(row == lane, line, 0.0), axis=1, keepdims=True)

    loaded("stream", "gain_in", "wf", "wq", "wk", "wv")
    stream = stream_ref[...].astype(f32)
    scaled = (stream * gain_in_ref[...].astype(f32)).astype(bf16)
    squares = jnp.sum(stream * stream, axis=1, keepdims=True)
    mine = low_half == (lax.rem(kv, 2) == 0)
    scaled_f = scaled.astype(f32)
    both = jnp.where(mine, jnp.concatenate([scaled_f, scaled_f], axis=1), 0.0).astype(bf16)
    part_f = lax.dot_general(both, wf[...], NT, preferred_element_type=f32)
    lane_f = lax.broadcasted_iota(jnp.int32, part_f.shape, 1)
    for r, w in enumerate((wq, wk, wv)):
        part = jnp.dot(scaled, w[...], preferred_element_type=f32)
        for h in range(HEADS):
            block = part[:, h * HD : (h + 1) * HD].reshape(SEQS // 4, 4, 128)
            if r == 0:
                send_qi[h * SEQS // 4 : (h + 1) * SEQS // 4] = block
            else:
                send_ri[h * SEQS // 4 : (h + 1) * SEQS // 4, r - 1] = block
    for h in range(HEADS):
        gate = jnp.sum(jnp.where(lane_f == tp * HEADS + h, part_f, 0.0), axis=1, keepdims=True)
        block = jnp.broadcast_to(gate, (SEQS, 128)).reshape(SEQS // 4, 4, 128)
        send_ri[h * SEQS // 4 : (h + 1) * SEQS // 4, 2] = block
    recv_qi[near] = send_qi[near]
    recv_ri[near] = send_ri[near]
    send_si[...] = as_row(squares)
    recv_si[near] = send_si[...]
    pl.semaphore_wait(barrier, NZ - 4 + GROUP - 1 + NTP - 1)
    to_group(SQ_IN, lambda to: send_si, recv_si.at[near])
    to_group(QUERY_IN, lambda to: send_qi.at[to], recv_qi.at[near])
    to_group(REST_IN, lambda to: send_ri.at[to], recv_ri.at[near])
    loaded("lengths", "decay")
    for s in range(SEQS):
        len_buf[s : s + 1, :] = jnp.full((1, 128), lengths_ref[s], jnp.int32)
    live = kv * POS + lane < len_buf[...]
    for h in range(HEADS):
        bias = jnp.where(live, decay_ref[:, h, :], MASKED)
        bias_buf[h * SEQS // NY : (h + 1) * SEQS // NY] = bias.reshape(SEQS // NY, NY, 128)
    loaded("keys", "values")
    arrived(SQ_IN, recv_si)
    send_fsi[...] = jnp.sum(recv_si[...], axis=0)
    recv_fsi[far] = send_fsi[...]
    to_far(FAR_SQ_IN, lambda to: send_fsi, recv_fsi.at[far])
    arrived(QUERY_IN, recv_qi)
    send_q[...] = jnp.sum(recv_qi[...], axis=0)
    recv_q[kv] = send_q[...]
    to_kv(QUERY, send_q, recv_q.at[kv])
    arrived(REST_IN, recv_ri)
    send_fr[...] = jnp.sum(recv_ri[...], axis=0)
    recv_fr[far] = send_fr[...]
    to_far(FAR_REST, lambda to: send_fr, recv_fr.at[far])
    arrived(FAR_SQ_IN, recv_fsi)
    scale_in = lax.rsqrt(as_column(jnp.sum(recv_fsi[...], axis=0)) / D + NORM_EPS)
    scale_rows = jnp.broadcast_to(scale_in, (SEQS, 128)).reshape(SEQS // 4, 4, 128)
    arrived(QUERY, recv_q)
    for h in range(HEADS):
        rows = 0.0
        for f in range(FARS):
            at = f * GROUP + h * SEQS // 4
            rows = rows + recv_q[at : at + SEQS // 4]
        rows = (rows * scale_rows).astype(bf16).astype(f32)
        query_buf[h * SEQS // 4 : (h + 1) * SEQS // 4] = rows
    score_scale = 1.0 / math.sqrt(HD)

    def part(steps):
        pairs = []
        for dz in steps:
            ring = lax.rem(z + dz, NZ)
            for j in range(NY):
                owner = ring * NY + j
                to, of = lax.rem(owner, GROUP), owner // GROUP
                at = (lax.rem(to, SEQS // 4) * 4 + of, to // (SEQS // 4))
                pairs.append((owner, to, of, at, dz, j))
        scores, biases = [], []
        for _, to, of, at, _, _ in pairs:
            q = query_buf[to, pl.ds(of, 1), :].astype(bf16)
            scores.append(lax.dot_general(q, keys[at], NT, preferred_element_type=f32))
            biases.append(bias_buf[to, pl.ds(of, 1), :])
        bias = jnp.concatenate(biases, axis=0)
        alive = bias > 0.5 * MASKED
        logits = jnp.concatenate(scores, axis=0) * score_scale + bias
        logits = jnp.where(alive, logits, MASKED)
        peak = jnp.max(logits, axis=1, keepdims=True)
        probs = jnp.where(alive, jnp.exp(logits - peak), 0.0)
        block_total = jnp.sum(probs, axis=1, keepdims=True)
        stats = jnp.where(low_half[: len(pairs)], peak, block_total)
        for k, (owner, _, _, at, _, _) in enumerate(pairs):
            send2[owner, 0:1, :] = jnp.dot(
                probs[k : k + 1].astype(bf16), values[at], preferred_element_type=f32
            )
            send2[owner, 1:2, :] = stats[k : k + 1]
        for owner, _, _, _, dz, j in pairs:
            send = lambda owner=owner: put(PART, send2.at[owner], recv2.at[kv], owner)
            if dz:
                send()
            else:
                pl.when(j != y)(send)

    part([8, 7, 9])
    part([6, 10, 5, 11])
    part([4, 12, 3, 13])
    part([2, 14, 1, 15, 0])
    recv2[kv] = send2[kv]
    arrived(FAR_REST, recv_fr)
    rest_buf[...] = jnp.sum(recv_fr[...], axis=0)
    lane_1 = lax.broadcasted_iota(jnp.int32, (1, 128), 1)
    my_seq = lax.rem(near, SEQS // 4) * 4 + far
    square_line = jnp.sum(recv_fsi[...], axis=0)
    square_sum = jnp.sum(jnp.where(lane_1 == my_seq, square_line, 0.0), axis=1, keepdims=True)
    my_scale = lax.rsqrt(square_sum / D + NORM_EPS)
    query = query_buf[near, pl.ds(far, 1), :]
    key_new = (rest_buf[0, pl.ds(far, 1), :] * my_scale).astype(bf16).astype(f32)
    value_new = (rest_buf[1, pl.ds(far, 1), :] * my_scale).astype(bf16).astype(f32)
    gate_in = rest_buf[2, pl.ds(far, 1), :][:, 0:1] * my_scale
    forget = jnp.minimum(gate_in, 0.0) - jnp.log1p(jnp.exp(-jnp.abs(gate_in)))
    own = jnp.sum(query * key_new, axis=1, keepdims=True) * score_scale
    arrived(PART, recv2)
    block_out, stats = recv2[:, 0, :], recv2[:, 1, :]
    low = lax.broadcasted_iota(jnp.int32, (NKV, 128), 1) < 64
    peaks = jnp.max(jnp.where(low, stats, 2 * MASKED), axis=1, keepdims=True)
    totals = jnp.max(jnp.where(low, 0.0, stats), axis=1, keepdims=True)
    own = own - forget
    top = jnp.maximum(own, jnp.max(peaks, axis=0, keepdims=True))
    weight = jnp.exp(peaks - top)
    own_weight = jnp.exp(own - top)
    numerator = jnp.sum(weight * block_out, axis=0, keepdims=True) + own_weight * value_new
    denominator = jnp.sum(weight * totals, axis=0, keepdims=True) + own_weight
    attended = numerator / denominator
    send_a[...] = attended
    my_pair = near * 4 + far
    recv_a[my_pair] = attended
    to_kv(ATT, send_a, recv_a.at[my_pair])
    loaded("wo", "gain_att", "gain_mlp", "wu", "wd")
    arrived(ATT, recv_a)

    part_out, att_squares = None, None
    for h in range(HEADS):
        att = recv_a[h * SEQS : (h + 1) * SEQS, 0, :]
        att_in = (att * gain_att_ref[h : h + 1, :].astype(f32)).astype(bf16)
        term = lax.dot_general(
            att_in, wo[:, h * HD : (h + 1) * HD], NT, preferred_element_type=f32
        )
        square = jnp.sum(att * att, axis=1, keepdims=True)
        part_out = term if h == 0 else part_out + term
        att_squares = square if h == 0 else att_squares + square
    half = SEQS // 2
    send_o[...] = jnp.concatenate([part_out[:half], part_out[half:]], axis=1)
    send_os[...] = as_row(att_squares)
    recv_o[tp] = send_o[...]
    recv_os[tp] = send_os[...]
    to_tp(OUT, send_o, recv_o.at[tp])
    to_tp(OUT_SQ, send_os, recv_os.at[tp])
    arrived(OUT, recv_o)
    arrived(OUT_SQ, recv_os)
    out_total = jnp.sum(recv_o[...], axis=0)
    out_total = jnp.concatenate([out_total[:, :COLS], out_total[:, COLS:]], axis=0)
    scale_att = lax.rsqrt(as_column(jnp.sum(recv_os[...], axis=0)) / HW + NORM_EPS)
    residual = (stream + scale_att * out_total).astype(bf16).astype(f32)

    mixer_in = (residual * gain_mlp_ref[...].astype(f32)).astype(bf16)
    send_sm[...] = as_row(jnp.sum(residual * residual, axis=1, keepdims=True))
    recv_sm[near] = send_sm[...]
    to_group(SQ_MIX, lambda to: send_sm, recv_sm.at[near])
    for u in range(BLOCKS):
        part = jnp.dot(mixer_in, wu[:, u * 128 : (u + 1) * 128], preferred_element_type=f32)
        send_u[u] = part.astype(bf16)
    recv_u[near] = send_u[near]
    to_group(UP, lambda to: send_u.at[to], recv_u.at[near])
    arrived(SQ_MIX, recv_sm)
    send_fsm[...] = jnp.sum(recv_sm[...], axis=0)
    recv_fsm[far] = send_fsm[...]
    to_far(FAR_SQ_MIX, lambda to: send_fsm, recv_fsm.at[far])
    arrived(UP, recv_u)
    group_sum = jnp.sum(recv_u[...].astype(f32), axis=0)
    send_fu[...] = group_sum.astype(bf16)
    recv_fu[far] = send_fu[...]
    to_far(FAR_UP, lambda to: send_fu, recv_fu.at[far])
    arrived(FAR_SQ_MIX, recv_fsm)
    scale_mixer = lax.rsqrt(as_column(jnp.sum(recv_fsm[...], axis=0)) / D + NORM_EPS)
    arrived(FAR_UP, recv_fu)
    active = jnp.maximum(jnp.sum(recv_fu[...].astype(f32), axis=0) * scale_mixer, 0.0)
    hidden = (active * active).astype(bf16)
    send_h[...] = hidden
    recv_h[near] = hidden
    to_group(HIDDEN, lambda to: send_h, recv_h.at[near])

    arrived(HIDDEN, recv_h)

    hidden_all = jnp.concatenate([recv_h[u] for u in range(BLOCKS)], axis=1)
    part_down = lax.dot_general(hidden_all, wd[...], NT, preferred_element_type=f32)
    send_d[...] = jnp.concatenate([part_down[:half], part_down[half:]], axis=1)
    recv_d[tp] = send_d[...]
    to_tp(DOWN, send_d, recv_d.at[tp])
    arrived(DOWN, recv_d)
    down = jnp.sum(recv_d[...], axis=0)
    down = jnp.concatenate([down[:, :COLS], down[:, COLS:]], axis=0)
    out_ref[...] = (residual + down).astype(bf16)

    for name, buffer in (
        (QUERY_IN, recv_qi), (REST_IN, recv_ri), (SQ_IN, recv_si), (FAR_SQ_IN, recv_fsi),
        (QUERY, recv_q), (FAR_REST, recv_fr),
        (PART, recv2), (ATT, recv_a), (OUT, recv_o), (OUT_SQ, recv_os), (UP, recv_u),
        (SQ_MIX, recv_sm), (FAR_UP, recv_fu), (FAR_SQ_MIX, recv_fsm), (HIDDEN, recv_h),
        (DOWN, recv_d),
    ):
        sent(name, buffer)


def per_device(
    stream, gain_in, w_query, w_key, w_value, w_forget, keys_cache, values_cache, decay_cache,
    lengths, gain_att, w_out, gain_mlp, w_up, w_down,
):
    hbm = pl.BlockSpec(memory_space=pl.ANY)
    V = pltpu.VMEM
    scratch = [
        V((SEQS, COLS), bf16), V((1, COLS), bf16),
        V((COLS, HEADS * HD), bf16), V((COLS, HEADS * HD), bf16), V((COLS, HEADS * HD), bf16),
        V((16, 128), bf16),
        V((SEQS, HEADS, POS, HD), bf16), V((SEQS, HEADS, POS, HD), bf16),
        V((SEQS, HEADS, POS), f32), pltpu.SMEM((SEQS,), jnp.int32), V((HEADS, HD), bf16),
        V((COLS, HEADS * HD), bf16), V((1, COLS), bf16), V((COLS, UNITS), bf16),
        V((COLS, UNITS), bf16),
        V((SEQS, 128), jnp.int32), V((NKV // 4, 4, 128), f32), V((NKV // 4, 4, 128), f32),
        V((GROUP, 4, 128), f32), V((GROUP, 4, 128), f32),
        V((GROUP, 3, 4, 128), f32), V((GROUP, 3, 4, 128), f32),
        V((1, 128), f32), V((GROUP, 1, 128), f32), V((1, 128), f32), V((FARS, 1, 128), f32),
        V((4, 128), f32), V((NKV, 4, 128), f32), V((3, 4, 128), f32), V((FARS, 3, 4, 128), f32),
        V((3, 4, 128), f32),
        V((NKV, 2, 128), f32), V((NKV, 2, 128), f32),
        V((1, 128), f32), V((NKV, 1, 128), f32),
        V((SEQS // 2, 128), f32), V((NTP, SEQS // 2, 128), f32),
        V((1, 128), f32), V((NTP, 1, 128), f32),
        V((BLOCKS, SEQS, 128), bf16), V((GROUP, SEQS, 128), bf16),
        V((1, 128), f32), V((GROUP, 1, 128), f32),
        V((SEQS, 128), bf16), V((FARS, SEQS, 128), bf16), V((1, 128), f32), V((FARS, 1, 128), f32),
        V((SEQS, 128), bf16), V((GROUP, SEQS, 128), bf16),
        V((SEQS // 2, 128), f32), V((NTP, SEQS // 2, 128), f32),
        pltpu.SemaphoreType.DMA((15,)),
        pltpu.SemaphoreType.DMA((EXCHANGES,)), pltpu.SemaphoreType.DMA((EXCHANGES,)),
    ]
    return pl.pallas_call(
        kernel,
        out_shape=pltpu.VMEM((SEQS, COLS), bf16),
        in_specs=[hbm] * 15,
        out_specs=pl.BlockSpec(memory_space=pltpu.VMEM),
        scratch_shapes=scratch,
        compiler_params=pltpu.CompilerParams(collective_id=0, has_side_effects=True),
    )(
        stream, gain_in.reshape(1, COLS), w_query, w_key, w_value, w_forget.T, keys_cache,
        values_cache, decay_cache, lengths, gain_att.reshape(HEADS, HD), w_out.T,
        gain_mlp.reshape(1, COLS), w_up, w_down.T,
    )


def solution(mesh):
    return jax.shard_map(
        per_device,
        mesh=mesh,
        in_specs=(
            P(None, "kv"), P("kv"), P("kv", "tp"), P("kv", "tp"), P("kv", "tp"), P(),
            P(None, "tp", "kv", None), P(None, "tp", "kv", None), P(None, "tp", "kv"), P(),
            P("tp"), P("tp", "kv"), P("kv"), P("kv", "tp"), P("tp", "kv"),
        ),
        out_specs=P(None, "kv"),
        check_vma=False,
    )
```

```python
import math

import jax
import jax.numpy as jnp
from jax import lax
from jax.experimental import pallas as pl
from jax.experimental.pallas import tpu as pltpu
from jax.sharding import PartitionSpec as P

f32, bf16 = jnp.float32, jnp.bfloat16
MESH = pl.DeviceIdType.MESH
NORM_EPS = 1e-06
MASKED = -1e30
NT = (((1,), (1,)), ((), ()))

NZ, NY, NTP = 16, 4, 8
NKV = NZ * NY
GROUP = 16
FARS = NKV // GROUP
SEQS, HEADS, HD, POS = 32, 2, 128, 128
COLS, UNITS = 64, 2048
D, HW = NKV * COLS, NTP * HEADS * HD
BLOCKS = UNITS // 128

(
    QUERY_IN, REST_IN, SQ_IN, FAR_SQ_IN, QUERY, FAR_REST, PART, ATT, OUT, OUT_SQ,
    UP, SQ_MIX, FAR_UP, FAR_SQ_MIX, HIDDEN, DOWN,
) = range(16)
EXCHANGES = 16
HOME = (FAR_SQ_IN, FAR_REST, OUT, OUT_SQ, FAR_UP, FAR_SQ_MIX, DOWN)


def kernel(
    stream_hbm, gain_in_hbm, wq_hbm, wk_hbm, wv_hbm, wf_hbm, keys_hbm, values_hbm, decay_hbm,
    lengths_hbm, gain_att_hbm, wo_hbm, gain_mlp_hbm, wu_hbm, wd_hbm,
    out_ref,
    stream_ref, gain_in_ref, wq, wk, wv, wf, keys, values, decay_ref, lengths_ref, gain_att_ref,
    wo, gain_mlp_ref, wu, wd,
    len_buf, bias_buf, query_buf,
    send_qi, recv_qi, send_ri, recv_ri, send_si, recv_si, send_fsi, recv_fsi, send_q, recv_q, send_fr, recv_fr, rest_buf,
    send2, recv2, send_a, recv_a, send_o, recv_o, send_os, recv_os,
    send_u, recv_u, send_sm, recv_sm, send_fu, recv_fu, send_fsm, recv_fsm, send_h, recv_h,
    send_d, recv_d,
    load_sem, send_sem, recv_sem, seen_sem, opposite_sem,
):
    kv, tp = lax.axis_index("kv"), lax.axis_index("tp")
    z, y = kv // NY, lax.rem(kv, NY)
    far, near = kv // GROUP, lax.rem(kv, GROUP)
    other = tp + 1 - 2 * lax.rem(tp, 2)

    def kv_peer(i):
        ring = i // NY
        dz = NZ // 2 + (1 - 2 * lax.rem(ring, 2)) * ((ring + 1) // 2)
        return lax.rem(z + dz, NZ) * NY + lax.rem(y + i, NY)

    def tp_peer(i):
        return lax.rem(tp + 1 + i, NTP)

    barrier = pltpu.get_barrier_semaphore()

    def greet(kv_to, tp_to):
        pl.semaphore_signal(barrier, 1, device_id=(kv_to, tp_to), device_id_type=MESH)

    def greet_group(i, c):
        greet(far * GROUP + lax.rem(near + 1 + i, GROUP), other)
        return c

    def greet_tp(i, c):
        greet(kv, tp_peer(i))
        return c

    after, before = lax.rem(kv + GROUP, NKV), lax.rem(kv + NKV - GROUP, NKV)
    greet(after, tp)
    greet(before, tp)
    lax.fori_loop(0, GROUP, greet_group, 0)
    lax.fori_loop(0, NTP - 1, greet_tp, 0)

    pair_cols = pl.ds(pl.multiple_of(kv // 2 * 128, 128), 128)
    loads = {
        "stream": (stream_hbm, stream_ref), "gain_in": (gain_in_hbm, gain_in_ref),
        "wf": (wf_hbm.at[:, pair_cols], wf), "wq": (wq_hbm, wq), "wk": (wk_hbm, wk),
        "wv": (wv_hbm, wv), "lengths": (lengths_hbm, lengths_ref),
        "decay": (decay_hbm, decay_ref), "keys": (keys_hbm, keys), "values": (values_hbm, values),
        "gain_att": (gain_att_hbm, gain_att_ref), "wo": (wo_hbm, wo),
        "gain_mlp": (gain_mlp_hbm, gain_mlp_ref), "wu": (wu_hbm, wu), "wd": (wd_hbm, wd),
    }
    loads = {
        name: pltpu.make_async_copy(a, b, load_sem.at[k])
        for k, (name, (a, b)) in enumerate(loads.items())
    }
    for load in loads.values():
        load.start()

    def loaded(*names):
        for name in names:
            loads[name].wait()

    lane = lax.broadcasted_iota(jnp.int32, (SEQS, 128), 1)
    low_half = lane < 64

    def put(name, source, target, peer, core):
        pltpu.make_async_remote_copy(
            src_ref=source, dst_ref=target, send_sem=send_sem.at[name],
            recv_sem=recv_sem.at[name], device_id=(peer, core), device_id_type=MESH,
        ).start()

    def to_kv(name, source, target):
        def step(i, c):
            put(name, source, target, kv_peer(i), other)
            return c

        lax.fori_loop(0, NKV, step, 0)

    def to_group(name, source, target):
        def step(i, c):
            to = lax.rem(near + 1 + i, GROUP)
            put(name, source(to), target, far * GROUP + to, other)
            return c

        lax.fori_loop(0, GROUP, step, 0)

    def to_far(name, source, target, steps=(2, 1, 3)):
        for i in steps:
            to = lax.rem(far + i, FARS)
            put(name, source(to), target, to * GROUP + near, tp)

    def to_tp(name, source, target):
        def step(i, c):
            pltpu.make_async_remote_copy(
                src_ref=source, dst_ref=target, send_sem=send_sem.at[name],
                recv_sem=recv_sem.at[name], device_id=(kv, tp_peer(i)), device_id_type=MESH,
            ).start()
            return c

        lax.fori_loop(0, NTP - 1, step, 0)

    def arrived(name, buffer):
        n = buffer.shape[0] - (name in HOME)
        whole = buffer.at[pl.ds(0, n)]
        pltpu.make_async_copy(whole, whole, recv_sem.at[name]).wait()

    def sent(name, buffer):
        n = buffer.shape[0] - (name in HOME)
        whole = buffer.at[pl.ds(0, n)]
        pltpu.make_async_copy(whole, whole, send_sem.at[name]).wait()

    row = lax.broadcasted_iota(jnp.int32, (SEQS, 128), 0)

    def as_row(column):
        return jnp.sum(jnp.where(row == lane, column, 0.0), axis=0, keepdims=True)

    def as_column(line):
        return jnp.sum(jnp.where(row == lane, line, 0.0), axis=1, keepdims=True)

    loaded("stream", "gain_in", "wf", "wq", "wk", "wv")
    stream = stream_ref[...].astype(f32)
    scaled = (stream * gain_in_ref[...].astype(f32)).astype(bf16)
    squares = jnp.sum(stream * stream, axis=1, keepdims=True)
    mine = low_half == (lax.rem(kv, 2) == 0)
    scaled_f = scaled.astype(f32)
    both = jnp.where(mine, jnp.concatenate([scaled_f, scaled_f], axis=1), 0.0).astype(bf16)
    part_f = lax.dot_general(both, wf[...], NT, preferred_element_type=f32)
    lane_f = lax.broadcasted_iota(jnp.int32, part_f.shape, 1)
    for r, w in enumerate((wq, wk, wv)):
        part = jnp.dot(scaled, w[...], preferred_element_type=f32)
        for h in range(HEADS):
            block = part[:, h * HD : (h + 1) * HD].reshape(SEQS // 4, 4, 128)
            if r == 0:
                send_qi[h * SEQS // 4 : (h + 1) * SEQS // 4] = block
            else:
                send_ri[h * SEQS // 4 : (h + 1) * SEQS // 4, r - 1] = block
    for h in range(HEADS):
        gate = jnp.sum(jnp.where(lane_f == tp * HEADS + h, part_f, 0.0), axis=1, keepdims=True)
        block = jnp.broadcast_to(gate, (SEQS, 128)).reshape(SEQS // 4, 4, 128)
        send_ri[h * SEQS // 4 : (h + 1) * SEQS // 4, 2] = block
    send_si[...] = as_row(squares)
    pl.semaphore_wait(barrier, 2 + GROUP + NTP - 1)
    for to in (after, before):
        pl.semaphore_signal(seen_sem, 1, device_id=(to, tp), device_id_type=MESH)
    to_group(SQ_IN, lambda to: send_si, recv_si.at[near])
    to_group(QUERY_IN, lambda to: send_qi.at[to], recv_qi.at[near])
    to_group(REST_IN, lambda to: send_ri.at[to], recv_ri.at[near])
    loaded("lengths", "decay")
    for s in range(SEQS):
        len_buf[s : s + 1, :] = jnp.full((1, 128), lengths_ref[s], jnp.int32)
    live = kv * POS + lane < len_buf[...]
    for h in range(HEADS):
        bias = jnp.where(live, decay_ref[:, h, :], MASKED)
        bias_buf[h * SEQS // NY : (h + 1) * SEQS // NY] = bias.reshape(SEQS // NY, NY, 128)
    loaded("keys", "values")
    pl.semaphore_wait(seen_sem, 2)
    pl.semaphore_signal(opposite_sem, 1, device_id=(before, tp), device_id_type=MESH)
    arrived(SQ_IN, recv_si)
    send_fsi[...] = jnp.sum(recv_si[...], axis=0)
    recv_fsi[far] = send_fsi[...]
    to_far(FAR_SQ_IN, lambda to: send_fsi, recv_fsi.at[far], (1, 3))
    arrived(QUERY_IN, recv_qi)
    send_q[...] = jnp.sum(recv_qi[...], axis=0)

    def beside(i, c):
        group = lax.rem(far + 1 + 2 * lax.rem(i, 2), FARS)
        put(QUERY, send_q, recv_q.at[kv], group * GROUP + i // 2, other)
        return c

    def across(i, c):
        put(QUERY, send_q, recv_q.at[kv], lax.rem(far + 2, FARS) * GROUP + i, other)
        return c

    pl.semaphore_wait(opposite_sem, 1)
    to_far(FAR_SQ_IN, lambda to: send_fsi, recv_fsi.at[far], (2,))
    to_kv(QUERY, send_q, recv_q.at[kv])
    arrived(REST_IN, recv_ri)
    send_fr[:3] = jnp.sum(recv_ri[...], axis=0)
    send_fr[3] = send_q[...]
    recv_fr[far] = send_fr[...]
    to_far(FAR_REST, lambda to: send_fr, recv_fr.at[far])
    arrived(FAR_SQ_IN, recv_fsi)
    scale_in = lax.rsqrt(as_column(jnp.sum(recv_fsi[...], axis=0)) / D + NORM_EPS)
    scale_rows = jnp.broadcast_to(scale_in, (SEQS, 128)).reshape(SEQS // 4, 4, 128)
    arrived(QUERY, recv_q)
    for h in range(HEADS):
        rows = 0.0
        for f in range(FARS):
            at = f * GROUP + h * SEQS // 4
            rows = rows + recv_q[at : at + SEQS // 4]
        rows = (rows * scale_rows).astype(bf16).astype(f32)
        query_buf[h * SEQS // 4 : (h + 1) * SEQS // 4] = rows
    score_scale = 1.0 / math.sqrt(HD)

    def part(steps):
        pairs = []
        for dz in steps:
            ring = lax.rem(z + dz, NZ)
            for j in range(NY):
                owner = ring * NY + j
                to, of = lax.rem(owner, GROUP), owner // GROUP
                at = (lax.rem(to, SEQS // 4) * 4 + of, to // (SEQS // 4))
                pairs.append((owner, to, of, at))
        scores, biases = [], []
        for _, to, of, at in pairs:
            q = query_buf[to, pl.ds(of, 1), :].astype(bf16)
            scores.append(lax.dot_general(q, keys[at], NT, preferred_element_type=f32))
            biases.append(bias_buf[to, pl.ds(of, 1), :])
        bias = jnp.concatenate(biases, axis=0)
        alive = bias > 0.5 * MASKED
        logits = jnp.concatenate(scores, axis=0) * score_scale + bias
        logits = jnp.where(alive, logits, MASKED)
        peak = jnp.max(logits, axis=1, keepdims=True)
        probs = jnp.where(alive, jnp.exp(logits - peak), 0.0)
        block_total = jnp.sum(probs, axis=1, keepdims=True)
        stats = jnp.where(low_half[: len(pairs)], peak, block_total)
        for k, (owner, _, _, at) in enumerate(pairs):
            send2[owner, 0:1, :] = jnp.dot(
                probs[k : k + 1].astype(bf16), values[at], preferred_element_type=f32
            )
            send2[owner, 1:2, :] = stats[k : k + 1]
        for owner, _, _, _ in pairs:
            put(PART, send2.at[owner], recv2.at[kv], owner, other)

    part([8, 7, 9])
    part([6, 10, 5, 11, 4, 12])
    part([3, 13, 2, 14, 1, 15, 0])
    arrived(FAR_REST, recv_fr)
    rest_buf[...] = jnp.sum(recv_fr[...], axis=0)
    lane_1 = lax.broadcasted_iota(jnp.int32, (1, 128), 1)
    my_seq = lax.rem(near, SEQS // 4) * 4 + far
    square_line = jnp.sum(recv_fsi[...], axis=0)
    square_sum = jnp.sum(jnp.where(lane_1 == my_seq, square_line, 0.0), axis=1, keepdims=True)
    my_scale = lax.rsqrt(square_sum / D + NORM_EPS)
    query = (rest_buf[3, pl.ds(far, 1), :] * my_scale).astype(bf16).astype(f32)
    key_new = (rest_buf[0, pl.ds(far, 1), :] * my_scale).astype(bf16).astype(f32)
    value_new = (rest_buf[1, pl.ds(far, 1), :] * my_scale).astype(bf16).astype(f32)
    gate_in = rest_buf[2, pl.ds(far, 1), :][:, 0:1] * my_scale
    forget = jnp.minimum(gate_in, 0.0) - jnp.log1p(jnp.exp(-jnp.abs(gate_in)))
    own = jnp.sum(query * key_new, axis=1, keepdims=True) * score_scale
    arrived(PART, recv2)
    block_out, stats = recv2[:, 0, :], recv2[:, 1, :]
    low = lax.broadcasted_iota(jnp.int32, (NKV, 128), 1) < 64
    peaks = jnp.max(jnp.where(low, stats, 2 * MASKED), axis=1, keepdims=True)
    totals = jnp.max(jnp.where(low, 0.0, stats), axis=1, keepdims=True)
    own = own - forget
    top = jnp.maximum(own, jnp.max(peaks, axis=0, keepdims=True))
    weight = jnp.exp(peaks - top)
    own_weight = jnp.exp(own - top)
    numerator = jnp.sum(weight * block_out, axis=0, keepdims=True) + own_weight * value_new
    denominator = jnp.sum(weight * totals, axis=0, keepdims=True) + own_weight
    attended = numerator / denominator
    send_a[...] = attended
    my_pair = near * 4 + far
    to_kv(ATT, send_a, recv_a.at[my_pair])
    loaded("wo", "gain_att", "gain_mlp", "wu", "wd")
    arrived(ATT, recv_a)

    part_out, att_squares = None, None
    for h in range(HEADS):
        att = recv_a[h * SEQS : (h + 1) * SEQS, 0, :]
        att_in = (att * gain_att_ref[h : h + 1, :].astype(f32)).astype(bf16)
        term = lax.dot_general(
            att_in, wo[:, h * HD : (h + 1) * HD], NT, preferred_element_type=f32
        )
        square = jnp.sum(att * att, axis=1, keepdims=True)
        part_out = term if h == 0 else part_out + term
        att_squares = square if h == 0 else att_squares + square
    half = SEQS // 2
    send_o[...] = jnp.concatenate([part_out[:half], part_out[half:]], axis=1)
    send_os[...] = as_row(att_squares)
    recv_o[tp] = send_o[...]
    recv_os[tp] = send_os[...]
    to_tp(OUT, send_o, recv_o.at[tp])
    to_tp(OUT_SQ, send_os, recv_os.at[tp])
    arrived(OUT, recv_o)
    arrived(OUT_SQ, recv_os)
    out_total = jnp.sum(recv_o[...], axis=0)
    out_total = jnp.concatenate([out_total[:, :COLS], out_total[:, COLS:]], axis=0)
    scale_att = lax.rsqrt(as_column(jnp.sum(recv_os[...], axis=0)) / HW + NORM_EPS)
    residual = (stream + scale_att * out_total).astype(bf16).astype(f32)

    mixer_in = (residual * gain_mlp_ref[...].astype(f32)).astype(bf16)
    send_sm[...] = as_row(jnp.sum(residual * residual, axis=1, keepdims=True))
    to_group(SQ_MIX, lambda to: send_sm, recv_sm.at[near])
    for u in range(BLOCKS):
        part = jnp.dot(mixer_in, wu[:, u * 128 : (u + 1) * 128], preferred_element_type=f32)
        send_u[u] = part.astype(bf16)
    to_group(UP, lambda to: send_u.at[to], recv_u.at[near])
    arrived(SQ_MIX, recv_sm)
    send_fsm[...] = jnp.sum(recv_sm[...], axis=0)
    recv_fsm[far] = send_fsm[...]
    to_far(FAR_SQ_MIX, lambda to: send_fsm, recv_fsm.at[far])
    arrived(UP, recv_u)
    group_sum = jnp.sum(recv_u[...].astype(f32), axis=0)
    send_fu[...] = group_sum.astype(bf16)
    recv_fu[far] = send_fu[...]
    to_far(FAR_UP, lambda to: send_fu, recv_fu.at[far])
    arrived(FAR_SQ_MIX, recv_fsm)
    scale_mixer = lax.rsqrt(as_column(jnp.sum(recv_fsm[...], axis=0)) / D + NORM_EPS)
    arrived(FAR_UP, recv_fu)
    active = jnp.maximum(jnp.sum(recv_fu[...].astype(f32), axis=0) * scale_mixer, 0.0)
    hidden = (active * active).astype(bf16)
    send_h[...] = hidden
    to_group(HIDDEN, lambda to: send_h, recv_h.at[near])

    arrived(HIDDEN, recv_h)

    hidden_all = jnp.concatenate([recv_h[u] for u in range(BLOCKS)], axis=1)
    part_down = lax.dot_general(hidden_all, wd[...], NT, preferred_element_type=f32)
    send_d[...] = jnp.concatenate([part_down[:half], part_down[half:]], axis=1)
    recv_d[tp] = send_d[...]
    to_tp(DOWN, send_d, recv_d.at[tp])
    arrived(DOWN, recv_d)
    down = jnp.sum(recv_d[...], axis=0)
    down = jnp.concatenate([down[:, :COLS], down[:, COLS:]], axis=0)
    out_ref[...] = (residual + down).astype(bf16)

    for name, buffer in (
        (QUERY_IN, recv_qi), (REST_IN, recv_ri), (SQ_IN, recv_si), (FAR_SQ_IN, recv_fsi),
        (QUERY, recv_q), (FAR_REST, recv_fr),
        (PART, recv2), (ATT, recv_a), (OUT, recv_o), (OUT_SQ, recv_os), (UP, recv_u),
        (SQ_MIX, recv_sm), (FAR_UP, recv_fu), (FAR_SQ_MIX, recv_fsm), (HIDDEN, recv_h),
        (DOWN, recv_d),
    ):
        sent(name, buffer)


def per_device(
    stream, gain_in, w_query, w_key, w_value, w_forget, keys_cache, values_cache, decay_cache,
    lengths, gain_att, w_out, gain_mlp, w_up, w_down,
):
    hbm = pl.BlockSpec(memory_space=pl.ANY)
    V = pltpu.VMEM
    scratch = [
        V((SEQS, COLS), bf16), V((1, COLS), bf16),
        V((COLS, HEADS * HD), bf16), V((COLS, HEADS * HD), bf16), V((COLS, HEADS * HD), bf16),
        V((16, 128), bf16),
        V((SEQS, HEADS, POS, HD), bf16), V((SEQS, HEADS, POS, HD), bf16),
        V((SEQS, HEADS, POS), f32), pltpu.SMEM((SEQS,), jnp.int32), V((HEADS, HD), bf16),
        V((COLS, HEADS * HD), bf16), V((1, COLS), bf16), V((COLS, UNITS), bf16),
        V((COLS, UNITS), bf16),
        V((SEQS, 128), jnp.int32), V((NKV // 4, 4, 128), f32), V((NKV // 4, 4, 128), f32),
        V((GROUP, 4, 128), f32), V((GROUP, 4, 128), f32),
        V((GROUP, 3, 4, 128), f32), V((GROUP, 3, 4, 128), f32),
        V((1, 128), f32), V((GROUP, 1, 128), f32), V((1, 128), f32), V((FARS, 1, 128), f32),
        V((4, 128), f32), V((NKV, 4, 128), f32), V((4, 4, 128), f32), V((FARS, 4, 4, 128), f32),
        V((4, 4, 128), f32),
        V((NKV, 2, 128), f32), V((NKV, 2, 128), f32),
        V((1, 128), f32), V((NKV, 1, 128), f32),
        V((SEQS // 2, 128), f32), V((NTP, SEQS // 2, 128), f32),
        V((1, 128), f32), V((NTP, 1, 128), f32),
        V((BLOCKS, SEQS, 128), bf16), V((GROUP, SEQS, 128), bf16),
        V((1, 128), f32), V((GROUP, 1, 128), f32),
        V((SEQS, 128), bf16), V((FARS, SEQS, 128), bf16), V((1, 128), f32), V((FARS, 1, 128), f32),
        V((SEQS, 128), bf16), V((GROUP, SEQS, 128), bf16),
        V((SEQS // 2, 128), f32), V((NTP, SEQS // 2, 128), f32),
        pltpu.SemaphoreType.DMA((15,)),
        pltpu.SemaphoreType.DMA((EXCHANGES,)), pltpu.SemaphoreType.DMA((EXCHANGES,)),
        pltpu.SemaphoreType.REGULAR, pltpu.SemaphoreType.REGULAR,
    ]
    return pl.pallas_call(
        kernel,
        out_shape=pltpu.VMEM((SEQS, COLS), bf16),
        in_specs=[hbm] * 15,
        out_specs=pl.BlockSpec(memory_space=pltpu.VMEM),
        scratch_shapes=scratch,
        compiler_params=pltpu.CompilerParams(collective_id=0, has_side_effects=True),
    )(
        stream, gain_in.reshape(1, COLS), w_query, w_key, w_value, w_forget.T, keys_cache,
        values_cache, decay_cache, lengths, gain_att.reshape(HEADS, HD), w_out.T,
        gain_mlp.reshape(1, COLS), w_up, w_down.T,
    )


def solution(mesh):
    return jax.shard_map(
        per_device,
        mesh=mesh,
        in_specs=(
            P(None, "kv"), P("kv"), P("kv", "tp"), P("kv", "tp"), P("kv", "tp"), P(),
            P(None, "tp", "kv", None), P(None, "tp", "kv", None), P(None, "tp", "kv"), P(),
            P("tp"), P("tp", "kv"), P("kv"), P("kv", "tp"), P("tp", "kv"),
        ),
        out_specs=P(None, "kv"),
        check_vma=False,
    )
```

```python
import math

import jax
import jax.numpy as jnp
from jax import lax
from jax.experimental import pallas as pl
from jax.experimental.pallas import tpu as pltpu
from jax.sharding import PartitionSpec as P

f32, bf16 = jnp.float32, jnp.bfloat16
MESH = pl.DeviceIdType.MESH
NORM_EPS = 1e-06
MASKED = -1e30
NT = (((1,), (1,)), ((), ()))

NZ, NY, NTP = 16, 4, 8
NKV = NZ * NY
GROUP = 16
FARS = NKV // GROUP
SEQS, HEADS, HD, POS = 32, 2, 128, 128
COLS, UNITS = 64, 2048
D, HW = NKV * COLS, NTP * HEADS * HD
BLOCKS = UNITS // 128

(
    QUERY_IN, REST_IN, SQ_IN, FAR_SQ_IN, QUERY, FAR_REST, PART, ATT, OUT, OUT_SQ,
    UP, SQ_MIX, FAR_UP, FAR_SQ_MIX, HIDDEN, DOWN,
) = range(16)
EXCHANGES = 16
HOME = (FAR_SQ_IN, FAR_REST, OUT, OUT_SQ, FAR_UP, FAR_SQ_MIX, DOWN)


def kernel(
    stream_hbm, gain_in_hbm, wq_hbm, wk_hbm, wv_hbm, wf_hbm, keys_hbm, values_hbm, decay_hbm,
    lengths_hbm, gain_att_hbm, wo_hbm, gain_mlp_hbm, wu_hbm, wd_hbm,
    out_ref,
    stream_ref, gain_in_ref, wq, wk, wv, wf, keys, values, decay_ref, lengths_ref, gain_att_ref,
    wo, gain_mlp_ref, wu, wd,
    len_buf, bias_buf, query_buf,
    send_qi, recv_qi, send_ri, recv_ri, send_si, recv_si, send_fsi, recv_fsi, send_q, recv_q, send_fr, recv_fr,
    send2, recv2, send_a, recv_a, send_o, recv_o, send_os, recv_os,
    send_u, recv_u, send_sm, recv_sm, send_fu, recv_fu, send_fsm, recv_fsm, send_h, recv_h,
    send_d, recv_d,
    load_sem, send_sem, recv_sem, seen_sem, opposite_sem,
):
    kv, tp = lax.axis_index("kv"), lax.axis_index("tp")
    z, y = kv // NY, lax.rem(kv, NY)
    far, near = kv // GROUP, lax.rem(kv, GROUP)
    other = tp + 1 - 2 * lax.rem(tp, 2)

    def kv_peer(i):
        ring = i // NY
        dz = NZ // 2 + (1 - 2 * lax.rem(ring, 2)) * ((ring + 1) // 2)
        return lax.rem(z + dz, NZ) * NY + lax.rem(y + i, NY)

    def tp_peer(i):
        return lax.rem(tp + 1 + i, NTP)

    barrier = pltpu.get_barrier_semaphore()

    def greet(kv_to, tp_to):
        pl.semaphore_signal(barrier, 1, device_id=(kv_to, tp_to), device_id_type=MESH)

    def greet_group(i, c):
        greet(far * GROUP + lax.rem(near + 1 + i, GROUP), other)
        return c

    def greet_tp(i, c):
        greet(kv, tp_peer(i))
        return c

    after, before = lax.rem(kv + GROUP, NKV), lax.rem(kv + NKV - GROUP, NKV)
    greet(after, tp)
    greet(before, tp)
    lax.fori_loop(0, GROUP, greet_group, 0)
    lax.fori_loop(0, NTP - 1, greet_tp, 0)

    pair_cols = pl.ds(pl.multiple_of(kv // 2 * 128, 128), 128)
    loads = {
        "stream": (stream_hbm, stream_ref), "gain_in": (gain_in_hbm, gain_in_ref),
        "wf": (wf_hbm.at[:, pair_cols], wf), "wq": (wq_hbm, wq), "wk": (wk_hbm, wk),
        "wv": (wv_hbm, wv), "lengths": (lengths_hbm, lengths_ref),
        "decay": (decay_hbm, decay_ref), "keys": (keys_hbm, keys), "values": (values_hbm, values),
        "gain_att": (gain_att_hbm, gain_att_ref), "wo": (wo_hbm, wo),
        "gain_mlp": (gain_mlp_hbm, gain_mlp_ref), "wu": (wu_hbm, wu), "wd": (wd_hbm, wd),
    }
    loads = {
        name: pltpu.make_async_copy(a, b, load_sem.at[k])
        for k, (name, (a, b)) in enumerate(loads.items())
    }
    for load in loads.values():
        load.start()

    def loaded(*names):
        for name in names:
            loads[name].wait()

    lane = lax.broadcasted_iota(jnp.int32, (SEQS, 128), 1)
    low_half = lane < 64

    def put(name, source, target, peer, core):
        pltpu.make_async_remote_copy(
            src_ref=source, dst_ref=target, send_sem=send_sem.at[name],
            recv_sem=recv_sem.at[name], device_id=(peer, core), device_id_type=MESH,
        ).start()

    def to_kv(name, source, target):
        def step(i, c):
            put(name, source, target, kv_peer(i), other)
            return c

        lax.fori_loop(0, NKV, step, 0)

    def to_group(name, source, target):
        def step(i, c):
            to = lax.rem(near + 1 + i, GROUP)
            put(name, source(to), target, far * GROUP + to, other)
            return c

        lax.fori_loop(0, GROUP, step, 0)

    def to_far(name, source, target, steps=(2, 1, 3)):
        for i in steps:
            to = lax.rem(far + i, FARS)
            put(name, source(to), target, to * GROUP + near, tp)

    def to_tp(name, source, target):
        def step(i, c):
            pltpu.make_async_remote_copy(
                src_ref=source, dst_ref=target, send_sem=send_sem.at[name],
                recv_sem=recv_sem.at[name], device_id=(kv, tp_peer(i)), device_id_type=MESH,
            ).start()
            return c

        lax.fori_loop(0, NTP - 1, step, 0)

    def arrived(name, buffer):
        n = buffer.shape[0] - (name in HOME)
        whole = buffer.at[pl.ds(0, n)]
        pltpu.make_async_copy(whole, whole, recv_sem.at[name]).wait()

    def sent(name, buffer):
        n = buffer.shape[0] - (name in HOME)
        whole = buffer.at[pl.ds(0, n)]
        pltpu.make_async_copy(whole, whole, send_sem.at[name]).wait()

    row = lax.broadcasted_iota(jnp.int32, (SEQS, 128), 0)

    def as_row(column):
        return jnp.sum(jnp.where(row == lane, column, 0.0), axis=0, keepdims=True)

    def as_column(line):
        return jnp.sum(jnp.where(row == lane, line, 0.0), axis=1, keepdims=True)

    loaded("stream", "gain_in", "wf", "wq", "wk", "wv")
    stream = stream_ref[...].astype(f32)
    scaled = (stream * gain_in_ref[...].astype(f32)).astype(bf16)
    squares = jnp.sum(stream * stream, axis=1, keepdims=True)
    mine = low_half == (lax.rem(kv, 2) == 0)
    scaled_f = scaled.astype(f32)
    both = jnp.where(mine, jnp.concatenate([scaled_f, scaled_f], axis=1), 0.0).astype(bf16)
    part_f = lax.dot_general(both, wf[...], NT, preferred_element_type=f32)
    lane_f = lax.broadcasted_iota(jnp.int32, part_f.shape, 1)
    for r, w in enumerate((wq, wk, wv)):
        part = jnp.dot(scaled, w[...], preferred_element_type=f32)
        for h in range(HEADS):
            block = part[:, h * HD : (h + 1) * HD].reshape(SEQS // 4, 4, 128)
            if r == 0:
                send_qi[h * SEQS // 4 : (h + 1) * SEQS // 4] = block
            else:
                send_ri[h * SEQS // 4 : (h + 1) * SEQS // 4, r - 1] = block
    for h in range(HEADS):
        gate = jnp.sum(jnp.where(lane_f == tp * HEADS + h, part_f, 0.0), axis=1, keepdims=True)
        block = jnp.broadcast_to(gate, (SEQS, 128)).reshape(SEQS // 4, 4, 128)
        send_ri[h * SEQS // 4 : (h + 1) * SEQS // 4, 2] = block
    send_si[...] = as_row(squares)
    pl.semaphore_wait(barrier, 2 + GROUP + NTP - 1)
    for to in (after, before):
        pl.semaphore_signal(seen_sem, 1, device_id=(to, tp), device_id_type=MESH)
    to_group(SQ_IN, lambda to: send_si, recv_si.at[near])
    to_group(QUERY_IN, lambda to: send_qi.at[to], recv_qi.at[near])
    to_group(REST_IN, lambda to: send_ri.at[to], recv_ri.at[near])
    loaded("lengths", "decay")
    for s in range(SEQS):
        len_buf[s : s + 1, :] = jnp.full((1, 128), lengths_ref[s], jnp.int32)
    live = kv * POS + lane < len_buf[...]
    for h in range(HEADS):
        bias = jnp.where(live, decay_ref[:, h, :], MASKED)
        bias_buf[h * SEQS // NY : (h + 1) * SEQS // NY] = bias.reshape(SEQS // NY, NY, 128)
    loaded("keys", "values")
    pl.semaphore_wait(seen_sem, 2)
    pl.semaphore_signal(opposite_sem, 1, device_id=(before, tp), device_id_type=MESH)
    arrived(SQ_IN, recv_si)
    send_fsi[...] = jnp.sum(recv_si[...], axis=0)
    recv_fsi[far] = send_fsi[...]
    to_far(FAR_SQ_IN, lambda to: send_fsi, recv_fsi.at[far], (1, 3))
    arrived(QUERY_IN, recv_qi)
    send_q[...] = jnp.sum(recv_qi[...], axis=0)

    def beside(i, c):
        group = lax.rem(far + 1 + 2 * lax.rem(i, 2), FARS)
        put(QUERY, send_q, recv_q.at[kv], group * GROUP + i // 2, other)
        return c

    def across(i, c):
        put(QUERY, send_q, recv_q.at[kv], lax.rem(far + 2, FARS) * GROUP + i, other)
        return c

    pl.semaphore_wait(opposite_sem, 1)
    to_far(FAR_SQ_IN, lambda to: send_fsi, recv_fsi.at[far], (2,))
    to_kv(QUERY, send_q, recv_q.at[kv])
    arrived(REST_IN, recv_ri)
    rest = jnp.sum(recv_ri[...], axis=0)
    for r in range(3):
        send_fr[:, r, :] = rest[r]
    send_fr[:, 3, :] = send_q[...]
    recv_fr[far] = send_fr[far]
    to_far(FAR_REST, lambda to: send_fr.at[to], recv_fr.at[far])
    arrived(FAR_SQ_IN, recv_fsi)
    scale_in = lax.rsqrt(as_column(jnp.sum(recv_fsi[...], axis=0)) / D + NORM_EPS)
    scale_rows = jnp.broadcast_to(scale_in, (SEQS, 128)).reshape(SEQS // 4, 4, 128)
    arrived(QUERY, recv_q)
    for h in range(HEADS):
        rows = 0.0
        for f in range(FARS):
            at = f * GROUP + h * SEQS // 4
            rows = rows + recv_q[at : at + SEQS // 4]
        rows = (rows * scale_rows).astype(bf16).astype(f32)
        query_buf[h * SEQS // 4 : (h + 1) * SEQS // 4] = rows
    score_scale = 1.0 / math.sqrt(HD)

    def part(steps):
        pairs = []
        for dz in steps:
            ring = lax.rem(z + dz, NZ)
            for j in range(NY):
                owner = ring * NY + j
                to, of = lax.rem(owner, GROUP), owner // GROUP
                at = (lax.rem(to, SEQS // 4) * 4 + of, to // (SEQS // 4))
                pairs.append((owner, to, of, at))
        scores, biases = [], []
        for _, to, of, at in pairs:
            q = query_buf[to, pl.ds(of, 1), :].astype(bf16)
            scores.append(lax.dot_general(q, keys[at], NT, preferred_element_type=f32))
            biases.append(bias_buf[to, pl.ds(of, 1), :])
        bias = jnp.concatenate(biases, axis=0)
        alive = bias > 0.5 * MASKED
        logits = jnp.concatenate(scores, axis=0) * score_scale + bias
        logits = jnp.where(alive, logits, MASKED)
        peak = jnp.max(logits, axis=1, keepdims=True)
        probs = jnp.where(alive, jnp.exp(logits - peak), 0.0)
        block_total = jnp.sum(probs, axis=1, keepdims=True)
        stats = jnp.where(low_half[: len(pairs)], peak, block_total)
        for k, (owner, _, _, at) in enumerate(pairs):
            send2[owner, 0:1, :] = jnp.dot(
                probs[k : k + 1].astype(bf16), values[at], preferred_element_type=f32
            )
            send2[owner, 1:2, :] = stats[k : k + 1]
        for owner, _, _, _ in pairs:
            put(PART, send2.at[owner], recv2.at[kv], owner, other)

    part([8, 7, 9])
    part([6, 10, 5, 11, 4, 12])
    part([3, 13, 2, 14, 1, 15, 0])
    arrived(FAR_REST, recv_fr)
    rest = jnp.sum(recv_fr[...], axis=0)
    lane_1 = lax.broadcasted_iota(jnp.int32, (1, 128), 1)
    my_seq = lax.rem(near, SEQS // 4) * 4 + far
    square_line = jnp.sum(recv_fsi[...], axis=0)
    square_sum = jnp.sum(jnp.where(lane_1 == my_seq, square_line, 0.0), axis=1, keepdims=True)
    my_scale = lax.rsqrt(square_sum / D + NORM_EPS)
    query = (rest[3:4, :] * my_scale).astype(bf16).astype(f32)
    key_new = (rest[0:1, :] * my_scale).astype(bf16).astype(f32)
    value_new = (rest[1:2, :] * my_scale).astype(bf16).astype(f32)
    gate_in = rest[2:3, 0:1] * my_scale
    forget = jnp.minimum(gate_in, 0.0) - jnp.log1p(jnp.exp(-jnp.abs(gate_in)))
    own = jnp.sum(query * key_new, axis=1, keepdims=True) * score_scale
    arrived(PART, recv2)
    block_out, stats = recv2[:, 0, :], recv2[:, 1, :]
    low = lax.broadcasted_iota(jnp.int32, (NKV, 128), 1) < 64
    peaks = jnp.max(jnp.where(low, stats, 2 * MASKED), axis=1, keepdims=True)
    totals = jnp.max(jnp.where(low, 0.0, stats), axis=1, keepdims=True)
    own = own - forget
    top = jnp.maximum(own, jnp.max(peaks, axis=0, keepdims=True))
    weight = jnp.exp(peaks - top)
    own_weight = jnp.exp(own - top)
    numerator = jnp.sum(weight * block_out, axis=0, keepdims=True) + own_weight * value_new
    denominator = jnp.sum(weight * totals, axis=0, keepdims=True) + own_weight
    attended = numerator / denominator
    send_a[...] = attended
    my_pair = near * 4 + far
    to_kv(ATT, send_a, recv_a.at[my_pair])
    loaded("wo", "gain_att", "gain_mlp", "wu", "wd")
    arrived(ATT, recv_a)

    part_out, att_squares = None, None
    for h in range(HEADS):
        att = recv_a[h * SEQS : (h + 1) * SEQS, 0, :]
        att_in = (att * gain_att_ref[h : h + 1, :].astype(f32)).astype(bf16)
        term = lax.dot_general(
            att_in, wo[:, h * HD : (h + 1) * HD], NT, preferred_element_type=f32
        )
        square = jnp.sum(att * att, axis=1, keepdims=True)
        part_out = term if h == 0 else part_out + term
        att_squares = square if h == 0 else att_squares + square
    half = SEQS // 2
    send_o[...] = jnp.concatenate([part_out[:half], part_out[half:]], axis=1)
    send_os[...] = as_row(att_squares)
    recv_o[tp] = send_o[...]
    recv_os[tp] = send_os[...]
    to_tp(OUT, send_o, recv_o.at[tp])
    to_tp(OUT_SQ, send_os, recv_os.at[tp])
    arrived(OUT, recv_o)
    arrived(OUT_SQ, recv_os)
    out_total = jnp.sum(recv_o[...], axis=0)
    out_total = jnp.concatenate([out_total[:, :COLS], out_total[:, COLS:]], axis=0)
    scale_att = lax.rsqrt(as_column(jnp.sum(recv_os[...], axis=0)) / HW + NORM_EPS)
    residual = (stream + scale_att * out_total).astype(bf16).astype(f32)

    mixer_in = (residual * gain_mlp_ref[...].astype(f32)).astype(bf16)
    send_sm[...] = as_row(jnp.sum(residual * residual, axis=1, keepdims=True))
    to_group(SQ_MIX, lambda to: send_sm, recv_sm.at[near])
    for u in range(BLOCKS):
        part = jnp.dot(mixer_in, wu[:, u * 128 : (u + 1) * 128], preferred_element_type=f32)
        send_u[u] = part.astype(bf16)
    to_group(UP, lambda to: send_u.at[to], recv_u.at[near])
    arrived(SQ_MIX, recv_sm)
    send_fsm[...] = jnp.sum(recv_sm[...], axis=0)
    recv_fsm[far] = send_fsm[...]
    to_far(FAR_SQ_MIX, lambda to: send_fsm, recv_fsm.at[far])
    arrived(UP, recv_u)
    group_sum = jnp.sum(recv_u[...].astype(f32), axis=0)
    send_fu[...] = group_sum.astype(bf16)
    recv_fu[far] = send_fu[...]
    to_far(FAR_UP, lambda to: send_fu, recv_fu.at[far])
    arrived(FAR_SQ_MIX, recv_fsm)
    scale_mixer = lax.rsqrt(as_column(jnp.sum(recv_fsm[...], axis=0)) / D + NORM_EPS)
    arrived(FAR_UP, recv_fu)
    active = jnp.maximum(jnp.sum(recv_fu[...].astype(f32), axis=0) * scale_mixer, 0.0)
    hidden = (active * active).astype(bf16)
    send_h[...] = hidden
    to_group(HIDDEN, lambda to: send_h, recv_h.at[near])

    arrived(HIDDEN, recv_h)

    hidden_all = jnp.concatenate([recv_h[u] for u in range(BLOCKS)], axis=1)
    part_down = lax.dot_general(hidden_all, wd[...], NT, preferred_element_type=f32)
    send_d[...] = jnp.concatenate([part_down[:half], part_down[half:]], axis=1)
    recv_d[tp] = send_d[...]
    to_tp(DOWN, send_d, recv_d.at[tp])
    arrived(DOWN, recv_d)
    down = jnp.sum(recv_d[...], axis=0)
    down = jnp.concatenate([down[:, :COLS], down[:, COLS:]], axis=0)
    out_ref[...] = (residual + down).astype(bf16)

    for name, buffer in (
        (QUERY_IN, recv_qi), (REST_IN, recv_ri), (SQ_IN, recv_si), (FAR_SQ_IN, recv_fsi),
        (QUERY, recv_q), (FAR_REST, recv_fr),
        (PART, recv2), (ATT, recv_a), (OUT, recv_o), (OUT_SQ, recv_os), (UP, recv_u),
        (SQ_MIX, recv_sm), (FAR_UP, recv_fu), (FAR_SQ_MIX, recv_fsm), (HIDDEN, recv_h),
        (DOWN, recv_d),
    ):
        sent(name, buffer)


def per_device(
    stream, gain_in, w_query, w_key, w_value, w_forget, keys_cache, values_cache, decay_cache,
    lengths, gain_att, w_out, gain_mlp, w_up, w_down,
):
    hbm = pl.BlockSpec(memory_space=pl.ANY)
    V = pltpu.VMEM
    scratch = [
        V((SEQS, COLS), bf16), V((1, COLS), bf16),
        V((COLS, HEADS * HD), bf16), V((COLS, HEADS * HD), bf16), V((COLS, HEADS * HD), bf16),
        V((16, 128), bf16),
        V((SEQS, HEADS, POS, HD), bf16), V((SEQS, HEADS, POS, HD), bf16),
        V((SEQS, HEADS, POS), f32), pltpu.SMEM((SEQS,), jnp.int32), V((HEADS, HD), bf16),
        V((COLS, HEADS * HD), bf16), V((1, COLS), bf16), V((COLS, UNITS), bf16),
        V((COLS, UNITS), bf16),
        V((SEQS, 128), jnp.int32), V((NKV // 4, 4, 128), f32), V((NKV // 4, 4, 128), f32),
        V((GROUP, 4, 128), f32), V((GROUP, 4, 128), f32),
        V((GROUP, 3, 4, 128), f32), V((GROUP, 3, 4, 128), f32),
        V((1, 128), f32), V((GROUP, 1, 128), f32), V((1, 128), f32), V((FARS, 1, 128), f32),
        V((4, 128), f32), V((NKV, 4, 128), f32), V((4, 4, 128), f32), V((FARS, 4, 128), f32),
        V((NKV, 2, 128), f32), V((NKV, 2, 128), f32),
        V((1, 128), f32), V((NKV, 1, 128), f32),
        V((SEQS // 2, 128), f32), V((NTP, SEQS // 2, 128), f32),
        V((1, 128), f32), V((NTP, 1, 128), f32),
        V((BLOCKS, SEQS, 128), bf16), V((GROUP, SEQS, 128), bf16),
        V((1, 128), f32), V((GROUP, 1, 128), f32),
        V((SEQS, 128), bf16), V((FARS, SEQS, 128), bf16), V((1, 128), f32), V((FARS, 1, 128), f32),
        V((SEQS, 128), bf16), V((GROUP, SEQS, 128), bf16),
        V((SEQS // 2, 128), f32), V((NTP, SEQS // 2, 128), f32),
        pltpu.SemaphoreType.DMA((15,)),
        pltpu.SemaphoreType.DMA((EXCHANGES,)), pltpu.SemaphoreType.DMA((EXCHANGES,)),
        pltpu.SemaphoreType.REGULAR, pltpu.SemaphoreType.REGULAR,
    ]
    return pl.pallas_call(
        kernel,
        out_shape=pltpu.VMEM((SEQS, COLS), bf16),
        in_specs=[hbm] * 15,
        out_specs=pl.BlockSpec(memory_space=pltpu.VMEM),
        scratch_shapes=scratch,
        compiler_params=pltpu.CompilerParams(collective_id=0, has_side_effects=True),
    )(
        stream, gain_in.reshape(1, COLS), w_query, w_key, w_value, w_forget.T, keys_cache,
        values_cache, decay_cache, lengths, gain_att.reshape(HEADS, HD), w_out.T,
        gain_mlp.reshape(1, COLS), w_up, w_down.T,
    )


def solution(mesh):
    return jax.shard_map(
        per_device,
        mesh=mesh,
        in_specs=(
            P(None, "kv"), P("kv"), P("kv", "tp"), P("kv", "tp"), P("kv", "tp"), P(),
            P(None, "tp", "kv", None), P(None, "tp", "kv", None), P(None, "tp", "kv"), P(),
            P("tp"), P("tp", "kv"), P("kv"), P("kv", "tp"), P("tp", "kv"),
        ),
        out_specs=P(None, "kv"),
        check_vma=False,
    )
```

```python
import math

import jax
import jax.numpy as jnp
from jax import lax
from jax.experimental import pallas as pl
from jax.experimental.pallas import tpu as pltpu
from jax.sharding import PartitionSpec as P

f32, bf16 = jnp.float32, jnp.bfloat16
MESH = pl.DeviceIdType.MESH
NORM_EPS = 1e-06
MASKED = -1e30
NT = (((1,), (1,)), ((), ()))

NZ, NY, NTP = 16, 4, 8
NKV = NZ * NY
GROUP = 16
FARS = NKV // GROUP
SEQS, HEADS, HD, POS = 32, 2, 128, 128
COLS, UNITS = 64, 2048
D, HW = NKV * COLS, NTP * HEADS * HD
BLOCKS = UNITS // 128

(
    QUERY_IN, REST_IN, SQ_IN, FAR_SQ_IN, QUERY, FAR_REST, PART, ATT, OUT, OUT_SQ,
    UP, SQ_MIX, FAR_UP, FAR_SQ_MIX, HIDDEN, DOWN,
) = range(16)
EXCHANGES = 16
HOME = (FAR_SQ_IN, FAR_REST, OUT, OUT_SQ, FAR_UP, FAR_SQ_MIX, DOWN)


def kernel(
    stream_hbm, gain_in_hbm, wq_hbm, wk_hbm, wv_hbm, wf_hbm, keys_hbm, values_hbm, decay_hbm,
    lengths_hbm, gain_att_hbm, wo_hbm, gain_mlp_hbm, wu_hbm, wd_hbm,
    out_ref,
    stream_ref, gain_in_ref, wq, wk, wv, wf, keys, values, decay_ref, lengths_ref, gain_att_ref,
    wo, gain_mlp_ref, wu, wd,
    len_buf, bias_buf, query_buf,
    send_qi, recv_qi, send_ri, recv_ri, send_si, recv_si, send_fsi, recv_fsi, send_q, recv_q, send_fr, recv_fr,
    send2, recv2, send_a, recv_a, send_o, recv_o, send_os, recv_os,
    send_u, recv_u, send_sm, recv_sm, send_fu, recv_fu, send_fsm, recv_fsm, send_h, recv_h,
    send_d, recv_d,
    load_sem, send_sem, recv_sem, seen_sem, opposite_sem,
):
    kv, tp = lax.axis_index("kv"), lax.axis_index("tp")
    z, y = kv // NY, lax.rem(kv, NY)
    far, near = kv // GROUP, lax.rem(kv, GROUP)
    other = tp + 1 - 2 * lax.rem(tp, 2)

    def kv_peer(i):
        ring = i // NY
        dz = NZ // 2 + (1 - 2 * lax.rem(ring, 2)) * ((ring + 1) // 2)
        return lax.rem(z + dz, NZ) * NY + lax.rem(y + i, NY)

    def tp_peer(i):
        return lax.rem(tp + 1 + i, NTP)

    barrier = pltpu.get_barrier_semaphore()

    def greet(kv_to, tp_to):
        pl.semaphore_signal(barrier, 1, device_id=(kv_to, tp_to), device_id_type=MESH)

    def greet_group(i, c):
        greet(far * GROUP + lax.rem(near + 1 + i, GROUP), other)
        return c

    def greet_tp(i, c):
        greet(kv, tp_peer(i))
        return c

    after, before = lax.rem(kv + GROUP, NKV), lax.rem(kv + NKV - GROUP, NKV)
    greet(after, tp)
    greet(before, tp)
    lax.fori_loop(0, GROUP, greet_group, 0)
    lax.fori_loop(0, NTP - 1, greet_tp, 0)

    pair_cols = pl.ds(pl.multiple_of(kv // 2 * 128, 128), 128)
    loads = {
        "stream": (stream_hbm, stream_ref), "gain_in": (gain_in_hbm, gain_in_ref),
        "wf": (wf_hbm.at[:, pair_cols], wf), "wq": (wq_hbm, wq), "wk": (wk_hbm, wk),
        "wv": (wv_hbm, wv), "lengths": (lengths_hbm, lengths_ref),
        "decay": (decay_hbm, decay_ref), "keys": (keys_hbm, keys), "values": (values_hbm, values),
        "gain_att": (gain_att_hbm, gain_att_ref), "wo": (wo_hbm, wo),
        "gain_mlp": (gain_mlp_hbm, gain_mlp_ref), "wu": (wu_hbm, wu), "wd": (wd_hbm, wd),
    }
    loads = {
        name: pltpu.make_async_copy(a, b, load_sem.at[k])
        for k, (name, (a, b)) in enumerate(loads.items())
    }
    for load in loads.values():
        load.start()

    def loaded(*names):
        for name in names:
            loads[name].wait()

    lane = lax.broadcasted_iota(jnp.int32, (SEQS, 128), 1)
    low_half = lane < 64

    def put(name, source, target, peer, core):
        pltpu.make_async_remote_copy(
            src_ref=source, dst_ref=target, send_sem=send_sem.at[name],
            recv_sem=recv_sem.at[name], device_id=(peer, core), device_id_type=MESH,
        ).start()

    def to_kv(name, source, target):
        def step(i, c):
            put(name, source, target, kv_peer(i), other)
            return c

        lax.fori_loop(0, NKV, step, 0)

    def to_group(name, source, target):
        def step(i, c):
            to = lax.rem(near + 1 + i, GROUP)
            put(name, source(to), target, far * GROUP + to, other)
            return c

        lax.fori_loop(0, GROUP, step, 0)

    def to_far(name, source, target, steps=(2, 1, 3)):
        for i in steps:
            to = lax.rem(far + i, FARS)
            put(name, source(to), target, to * GROUP + near, tp)

    def to_tp(name, source, target):
        def step(i, c):
            pltpu.make_async_remote_copy(
                src_ref=source, dst_ref=target, send_sem=send_sem.at[name],
                recv_sem=recv_sem.at[name], device_id=(kv, tp_peer(i)), device_id_type=MESH,
            ).start()
            return c

        lax.fori_loop(0, NTP - 1, step, 0)

    def arrived(name, buffer):
        n = buffer.shape[0] - (name in HOME)
        whole = buffer.at[pl.ds(0, n)]
        pltpu.make_async_copy(whole, whole, recv_sem.at[name]).wait()

    def sent(name, buffer):
        n = buffer.shape[0] - (name in HOME)
        whole = buffer.at[pl.ds(0, n)]
        pltpu.make_async_copy(whole, whole, send_sem.at[name]).wait()

    row = lax.broadcasted_iota(jnp.int32, (SEQS, 128), 0)

    def as_row(column):
        return jnp.sum(jnp.where(row == lane, column, 0.0), axis=0, keepdims=True)

    def as_column(line):
        return jnp.sum(jnp.where(row == lane, line, 0.0), axis=1, keepdims=True)

    loaded("stream", "gain_in", "wf", "wq", "wk", "wv")
    stream = stream_ref[...].astype(f32)
    scaled = (stream * gain_in_ref[...].astype(f32)).astype(bf16)
    squares = jnp.sum(stream * stream, axis=1, keepdims=True)
    mine = low_half == (lax.rem(kv, 2) == 0)
    scaled_f = scaled.astype(f32)
    both = jnp.where(mine, jnp.concatenate([scaled_f, scaled_f], axis=1), 0.0).astype(bf16)
    part_f = lax.dot_general(both, wf[...], NT, preferred_element_type=f32)
    lane_f = lax.broadcasted_iota(jnp.int32, part_f.shape, 1)
    for r, w in enumerate((wq, wk, wv)):
        part = jnp.dot(scaled, w[...], preferred_element_type=f32)
        for h in range(HEADS):
            block = part[:, h * HD : (h + 1) * HD].reshape(SEQS // 4, 4, 128)
            if r == 0:
                send_qi[h * SEQS // 4 : (h + 1) * SEQS // 4] = block
            else:
                send_ri[h * SEQS // 4 : (h + 1) * SEQS // 4, r - 1] = block
    for h in range(HEADS):
        gate = jnp.sum(jnp.where(lane_f == tp * HEADS + h, part_f, 0.0), axis=1, keepdims=True)
        block = jnp.broadcast_to(gate, (SEQS, 128)).reshape(SEQS // 4, 4, 128)
        send_ri[h * SEQS // 4 : (h + 1) * SEQS // 4, 2] = block
    send_si[...] = as_row(squares)
    pl.semaphore_wait(barrier, 2 + GROUP + NTP - 1)
    for to in (after, before):
        pl.semaphore_signal(seen_sem, 1, device_id=(to, tp), device_id_type=MESH)
    to_group(SQ_IN, lambda to: send_si, recv_si.at[near])
    to_group(QUERY_IN, lambda to: send_qi.at[to], recv_qi.at[near])
    to_group(REST_IN, lambda to: send_ri.at[to], recv_ri.at[near])
    loaded("lengths", "decay")
    for s in range(SEQS):
        len_buf[s : s + 1, :] = jnp.full((1, 128), lengths_ref[s], jnp.int32)
    live = kv * POS + lane < len_buf[...]
    for h in range(HEADS):
        bias = jnp.where(live, decay_ref[:, h, :], MASKED)
        bias_buf[h * SEQS // NY : (h + 1) * SEQS // NY] = bias.reshape(SEQS // NY, NY, 128)
    loaded("keys", "values")
    pl.semaphore_wait(seen_sem, 2)
    pl.semaphore_signal(opposite_sem, 1, device_id=(before, tp), device_id_type=MESH)
    arrived(SQ_IN, recv_si)
    send_fsi[...] = jnp.sum(recv_si[...], axis=0)
    recv_fsi[far] = send_fsi[...]
    to_far(FAR_SQ_IN, lambda to: send_fsi, recv_fsi.at[far], (1, 3))
    arrived(QUERY_IN, recv_qi)
    send_q[...] = jnp.sum(recv_qi[...], axis=0)

    def beside(i, c):
        group = lax.rem(far + 1 + 2 * lax.rem(i, 2), FARS)
        put(QUERY, send_q, recv_q.at[kv], group * GROUP + i // 2, other)
        return c

    def across(i, c):
        put(QUERY, send_q, recv_q.at[kv], lax.rem(far + 2, FARS) * GROUP + i, other)
        return c

    pl.semaphore_wait(opposite_sem, 1)
    to_far(FAR_SQ_IN, lambda to: send_fsi, recv_fsi.at[far], (2,))
    to_kv(QUERY, send_q, recv_q.at[kv])
    arrived(FAR_SQ_IN, recv_fsi)
    scale_in = lax.rsqrt(as_column(jnp.sum(recv_fsi[...], axis=0)) / D + NORM_EPS)
    scale_rows = jnp.broadcast_to(scale_in, (SEQS, 128)).reshape(SEQS // 4, 4, 128)
    arrived(QUERY, recv_q)
    for h in range(HEADS):
        rows = 0.0
        for f in range(FARS):
            at = f * GROUP + h * SEQS // 4
            rows = rows + recv_q[at : at + SEQS // 4]
        rows = (rows * scale_rows).astype(bf16).astype(f32)
        query_buf[h * SEQS // 4 : (h + 1) * SEQS // 4] = rows
    score_scale = 1.0 / math.sqrt(HD)

    def part(steps):
        pairs = []
        for dz in steps:
            ring = lax.rem(z + dz, NZ)
            for j in range(NY):
                owner = ring * NY + j
                to, of = lax.rem(owner, GROUP), owner // GROUP
                at = (lax.rem(to, SEQS // 4) * 4 + of, to // (SEQS // 4))
                pairs.append((owner, to, of, at))
        scores, biases = [], []
        for _, to, of, at in pairs:
            q = query_buf[to, pl.ds(of, 1), :].astype(bf16)
            scores.append(lax.dot_general(q, keys[at], NT, preferred_element_type=f32))
            biases.append(bias_buf[to, pl.ds(of, 1), :])
        bias = jnp.concatenate(biases, axis=0)
        alive = bias > 0.5 * MASKED
        logits = jnp.concatenate(scores, axis=0) * score_scale + bias
        logits = jnp.where(alive, logits, MASKED)
        peak = jnp.max(logits, axis=1, keepdims=True)
        probs = jnp.where(alive, jnp.exp(logits - peak), 0.0)
        block_total = jnp.sum(probs, axis=1, keepdims=True)
        stats = jnp.where(low_half[: len(pairs)], peak, block_total)
        for k, (owner, _, _, at) in enumerate(pairs):
            send2[owner, 0:1, :] = jnp.dot(
                probs[k : k + 1].astype(bf16), values[at], preferred_element_type=f32
            )
            send2[owner, 1:2, :] = stats[k : k + 1]
        for owner, _, _, _ in pairs:
            put(PART, send2.at[owner], recv2.at[kv], owner, other)

    part([8, 7, 9])
    arrived(REST_IN, recv_ri)
    rest = jnp.sum(recv_ri[...], axis=0)
    for r in range(3):
        send_fr[:, r, :] = rest[r]
    send_fr[:, 3, :] = send_q[...]
    recv_fr[far] = send_fr[far]
    to_far(FAR_REST, lambda to: send_fr.at[to], recv_fr.at[far])
    part([6, 10, 5, 11, 4, 12])
    part([3, 13, 2, 14, 1, 15, 0])
    arrived(FAR_REST, recv_fr)
    rest = jnp.sum(recv_fr[...], axis=0)
    lane_1 = lax.broadcasted_iota(jnp.int32, (1, 128), 1)
    my_seq = lax.rem(near, SEQS // 4) * 4 + far
    square_line = jnp.sum(recv_fsi[...], axis=0)
    square_sum = jnp.sum(jnp.where(lane_1 == my_seq, square_line, 0.0), axis=1, keepdims=True)
    my_scale = lax.rsqrt(square_sum / D + NORM_EPS)
    query = (rest[3:4, :] * my_scale).astype(bf16).astype(f32)
    key_new = (rest[0:1, :] * my_scale).astype(bf16).astype(f32)
    value_new = (rest[1:2, :] * my_scale).astype(bf16).astype(f32)
    gate_in = rest[2:3, 0:1] * my_scale
    forget = jnp.minimum(gate_in, 0.0) - jnp.log1p(jnp.exp(-jnp.abs(gate_in)))
    own = jnp.sum(query * key_new, axis=1, keepdims=True) * score_scale
    arrived(PART, recv2)
    block_out, stats = recv2[:, 0, :], recv2[:, 1, :]
    low = lax.broadcasted_iota(jnp.int32, (NKV, 128), 1) < 64
    peaks = jnp.max(jnp.where(low, stats, 2 * MASKED), axis=1, keepdims=True)
    totals = jnp.max(jnp.where(low, 0.0, stats), axis=1, keepdims=True)
    own = own - forget
    top = jnp.maximum(own, jnp.max(peaks, axis=0, keepdims=True))
    weight = jnp.exp(peaks - top)
    own_weight = jnp.exp(own - top)
    numerator = jnp.sum(weight * block_out, axis=0, keepdims=True) + own_weight * value_new
    denominator = jnp.sum(weight * totals, axis=0, keepdims=True) + own_weight
    attended = numerator / denominator
    send_a[...] = attended
    my_pair = near * 4 + far
    to_kv(ATT, send_a, recv_a.at[my_pair])
    loaded("wo", "gain_att", "gain_mlp", "wu", "wd")
    arrived(ATT, recv_a)

    part_out, att_squares = None, None
    for h in range(HEADS):
        att = recv_a[h * SEQS : (h + 1) * SEQS, 0, :]
        att_in = (att * gain_att_ref[h : h + 1, :].astype(f32)).astype(bf16)
        term = lax.dot_general(
            att_in, wo[:, h * HD : (h + 1) * HD], NT, preferred_element_type=f32
        )
        square = jnp.sum(att * att, axis=1, keepdims=True)
        part_out = term if h == 0 else part_out + term
        att_squares = square if h == 0 else att_squares + square
    half = SEQS // 2
    send_o[...] = jnp.concatenate([part_out[:half], part_out[half:]], axis=1)
    send_os[...] = as_row(att_squares)
    recv_o[tp] = send_o[...]
    recv_os[tp] = send_os[...]
    to_tp(OUT, send_o, recv_o.at[tp])
    to_tp(OUT_SQ, send_os, recv_os.at[tp])
    arrived(OUT, recv_o)
    arrived(OUT_SQ, recv_os)
    out_total = jnp.sum(recv_o[...], axis=0)
    out_total = jnp.concatenate([out_total[:, :COLS], out_total[:, COLS:]], axis=0)
    scale_att = lax.rsqrt(as_column(jnp.sum(recv_os[...], axis=0)) / HW + NORM_EPS)
    residual = (stream + scale_att * out_total).astype(bf16).astype(f32)

    mixer_in = (residual * gain_mlp_ref[...].astype(f32)).astype(bf16)
    send_sm[...] = as_row(jnp.sum(residual * residual, axis=1, keepdims=True))
    to_group(SQ_MIX, lambda to: send_sm, recv_sm.at[near])
    for u in range(BLOCKS):
        part = jnp.dot(mixer_in, wu[:, u * 128 : (u + 1) * 128], preferred_element_type=f32)
        send_u[u] = part.astype(bf16)
    to_group(UP, lambda to: send_u.at[to], recv_u.at[near])
    arrived(SQ_MIX, recv_sm)
    send_fsm[...] = jnp.sum(recv_sm[...], axis=0)
    recv_fsm[far] = send_fsm[...]
    to_far(FAR_SQ_MIX, lambda to: send_fsm, recv_fsm.at[far])
    arrived(UP, recv_u)
    group_sum = jnp.sum(recv_u[...].astype(f32), axis=0)
    send_fu[...] = group_sum.astype(bf16)
    recv_fu[far] = send_fu[...]
    to_far(FAR_UP, lambda to: send_fu, recv_fu.at[far])
    arrived(FAR_SQ_MIX, recv_fsm)
    scale_mixer = lax.rsqrt(as_column(jnp.sum(recv_fsm[...], axis=0)) / D + NORM_EPS)
    arrived(FAR_UP, recv_fu)
    active = jnp.maximum(jnp.sum(recv_fu[...].astype(f32), axis=0) * scale_mixer, 0.0)
    hidden = (active * active).astype(bf16)
    send_h[...] = hidden
    to_group(HIDDEN, lambda to: send_h, recv_h.at[near])

    arrived(HIDDEN, recv_h)

    hidden_all = jnp.concatenate([recv_h[u] for u in range(BLOCKS)], axis=1)
    part_down = lax.dot_general(hidden_all, wd[...], NT, preferred_element_type=f32)
    send_d[...] = jnp.concatenate([part_down[:half], part_down[half:]], axis=1)
    recv_d[tp] = send_d[...]
    to_tp(DOWN, send_d, recv_d.at[tp])
    arrived(DOWN, recv_d)
    down = jnp.sum(recv_d[...], axis=0)
    down = jnp.concatenate([down[:, :COLS], down[:, COLS:]], axis=0)
    out_ref[...] = (residual + down).astype(bf16)

    for name, buffer in (
        (QUERY_IN, recv_qi), (REST_IN, recv_ri), (SQ_IN, recv_si), (FAR_SQ_IN, recv_fsi),
        (QUERY, recv_q), (FAR_REST, recv_fr),
        (PART, recv2), (ATT, recv_a), (OUT, recv_o), (OUT_SQ, recv_os), (UP, recv_u),
        (SQ_MIX, recv_sm), (FAR_UP, recv_fu), (FAR_SQ_MIX, recv_fsm), (HIDDEN, recv_h),
        (DOWN, recv_d),
    ):
        sent(name, buffer)


def per_device(
    stream, gain_in, w_query, w_key, w_value, w_forget, keys_cache, values_cache, decay_cache,
    lengths, gain_att, w_out, gain_mlp, w_up, w_down,
):
    hbm = pl.BlockSpec(memory_space=pl.ANY)
    V = pltpu.VMEM
    scratch = [
        V((SEQS, COLS), bf16), V((1, COLS), bf16),
        V((COLS, HEADS * HD), bf16), V((COLS, HEADS * HD), bf16), V((COLS, HEADS * HD), bf16),
        V((16, 128), bf16),
        V((SEQS, HEADS, POS, HD), bf16), V((SEQS, HEADS, POS, HD), bf16),
        V((SEQS, HEADS, POS), f32), pltpu.SMEM((SEQS,), jnp.int32), V((HEADS, HD), bf16),
        V((COLS, HEADS * HD), bf16), V((1, COLS), bf16), V((COLS, UNITS), bf16),
        V((COLS, UNITS), bf16),
        V((SEQS, 128), jnp.int32), V((NKV // 4, 4, 128), f32), V((NKV // 4, 4, 128), f32),
        V((GROUP, 4, 128), f32), V((GROUP, 4, 128), f32),
        V((GROUP, 3, 4, 128), f32), V((GROUP, 3, 4, 128), f32),
        V((1, 128), f32), V((GROUP, 1, 128), f32), V((1, 128), f32), V((FARS, 1, 128), f32),
        V((4, 128), f32), V((NKV, 4, 128), f32), V((4, 4, 128), f32), V((FARS, 4, 128), f32),
        V((NKV, 2, 128), f32), V((NKV, 2, 128), f32),
        V((1, 128), f32), V((NKV, 1, 128), f32),
        V((SEQS // 2, 128), f32), V((NTP, SEQS // 2, 128), f32),
        V((1, 128), f32), V((NTP, 1, 128), f32),
        V((BLOCKS, SEQS, 128), bf16), V((GROUP, SEQS, 128), bf16),
        V((1, 128), f32), V((GROUP, 1, 128), f32),
        V((SEQS, 128), bf16), V((FARS, SEQS, 128), bf16), V((1, 128), f32), V((FARS, 1, 128), f32),
        V((SEQS, 128), bf16), V((GROUP, SEQS, 128), bf16),
        V((SEQS // 2, 128), f32), V((NTP, SEQS // 2, 128), f32),
        pltpu.SemaphoreType.DMA((15,)),
        pltpu.SemaphoreType.DMA((EXCHANGES,)), pltpu.SemaphoreType.DMA((EXCHANGES,)),
        pltpu.SemaphoreType.REGULAR, pltpu.SemaphoreType.REGULAR,
    ]
    return pl.pallas_call(
        kernel,
        out_shape=pltpu.VMEM((SEQS, COLS), bf16),
        in_specs=[hbm] * 15,
        out_specs=pl.BlockSpec(memory_space=pltpu.VMEM),
        scratch_shapes=scratch,
        compiler_params=pltpu.CompilerParams(collective_id=0, has_side_effects=True),
    )(
        stream, gain_in.reshape(1, COLS), w_query, w_key, w_value, w_forget.T, keys_cache,
        values_cache, decay_cache, lengths, gain_att.reshape(HEADS, HD), w_out.T,
        gain_mlp.reshape(1, COLS), w_up, w_down.T,
    )


def solution(mesh):
    return jax.shard_map(
        per_device,
        mesh=mesh,
        in_specs=(
            P(None, "kv"), P("kv"), P("kv", "tp"), P("kv", "tp"), P("kv", "tp"), P(),
            P(None, "tp", "kv", None), P(None, "tp", "kv", None), P(None, "tp", "kv"), P(),
            P("tp"), P("tp", "kv"), P("kv"), P("kv", "tp"), P("tp", "kv"),
        ),
        out_specs=P(None, "kv"),
        check_vma=False,
    )
```
